512 devices in a mesh: sp: 64 (over z, y), tp: 8 (over x, core).
Axes of the slice: x: 4, y: 8, z: 8, core: 2. Of those that a mesh axis runs over, the one named last changes fastest.
Arguments:
- latent: bfloat16 [16384, 2048], P(('sp', 'tp')), may hold values from -6 to 6
- context: bfloat16 [512, 2048], P('sp'), may hold values from -6 to 6
- condition: float32 [2048], P('tp'), may hold values from -6 to 6
- context_condition: float32 [2048], P('tp'), may hold values from -6 to 6
- modulation_weight: bfloat16 [2048, 6144], P('tp', 'sp'), may hold values from -0.125 to 0.125
- query_first: bfloat16 [2048, 512], P(None, 'tp'), may hold values from -1 to 1
- query_second: bfloat16 [2048, 512], P(None, 'tp'), may hold values from -1 to 1
- key_first: bfloat16 [2048, 512], P(None, 'tp'), may hold values from -1 to 1
- key_second: bfloat16 [2048, 512], P(None, 'tp'), may hold values from -1 to 1
- value_weight: bfloat16 [2048, 1024], P(None, 'tp'), may hold values from -0.125 to 0.125
- lambda_head: float32 [8], P('tp'), may hold values from 0.3 to 0.8
- context_score_boost: float32 [8], P('tp'), may hold values from 1.5 to 3
- head_gain: float32 [128], replicated, may hold values from 0.1 to 1.9
- output_weight: bfloat16 [1024, 2048], P('tp'), may hold values from -0.1875 to 0.1875
Outputs:
- updated: bfloat16 [16384, 2048], P(('sp', 'tp'))
The draws below stay inside these ranges and needn't reach their ends.
All inputs are finite; a program needn't handle non-finite values.
Results may differ from the reference program's by a relative error of at most 0.0095.
Values may be sent and summed in bfloat16 or wider, within the bound.
A program may use at most 64 MiB of HBM per device.

```python
import jax
import jax.numpy as jnp
from jax import lax

D = 2048
HEADS = 8
HEAD_DIM = 64
VALUE_DIM = 128
GRID_W = 64
CTX = 512
TOKENS = 16384


def drawn_weight(key, stream):
    jitter = jax.random.normal(jax.random.fold_in(key, stream), (D, HEADS * HEAD_DIM), jnp.float32)
    return jnp.clip(jitter, -6.0, 6.0) * D ** (-0.5)


def draw_latent(key, part):
    jitter = jax.random.normal(jax.random.fold_in(key, 21), (TOKENS, D), jnp.float32)
    result = jnp.clip(jitter, -6.0, 6.0)
    return result.astype(jnp.bfloat16)


def draw_query_first(key, part):
    result = drawn_weight(key, 31)
    return jnp.clip(result, -1.0, 1.0).astype(jnp.bfloat16)


def draw_key_first(key, part):
    result = drawn_weight(key, 32)
    return jnp.clip(result, -1.0, 1.0).astype(jnp.bfloat16)


def draw_query_second(key, part):
    result = drawn_weight(key, 33)
    return jnp.clip(result, -1.0, 1.0).astype(jnp.bfloat16)


def draw_key_second(key, part):
    result = drawn_weight(key, 34)
    return jnp.clip(result, -1.0, 1.0).astype(jnp.bfloat16)


def shard_levels(stream_key, extent, cuts, smallest, largest):
    def one(position, shards_of):
        draws = jax.random.uniform(jax.random.fold_in(jax.random.fold_in(stream_key, 6), position), (shards_of,), jnp.float32, smallest / len(cuts), largest / len(cuts))
        return jnp.repeat(jnp.exp(draws), extent[position] // shards_of).reshape((-1,) + (1,) * (len(extent) - position - 1))

    factor_of = one(*cuts[0])
    for cut in cuts[1:]:
        factor_of = factor_of * one(*cut)
    return factor_of


def gaussian(stream_key, dims, scale, limit, split=(), kind=jnp.bfloat16):
    loudness = shard_levels(stream_key, dims, split, -0.22, 0.18) if split else 1.0
    values = jax.random.normal(stream_key, dims, jnp.float32) * scale * loudness
    return jnp.minimum(jnp.maximum(values, -limit), limit).astype(kind)


def setup_inputs(seed: int = 0) -> dict:
    key_list = jax.random.split(jax.random.key(seed), 15)
    latent = draw_latent(jax.random.fold_in(key_list[14], 71), 0)
    context = gaussian(key_list[1], (CTX, D), 1.0, 6.0, ((0, 64),))
    condition = gaussian(key_list[2], (D,), 1.0, 6.0, ((0, 8),), jnp.float32)
    context_condition = gaussian(key_list[3], (D,), 1.0, 6.0, ((0, 8),), jnp.float32)
    modulation_weight = gaussian(key_list[4], (D, 3 * D), D ** -0.5, 0.125, ((0, 8), (1, 64)))
    query_first = draw_query_first(jax.random.fold_in(key_list[14], 71), 0)
    query_second = draw_query_second(jax.random.fold_in(key_list[14], 71), 0)
    key_first = draw_key_first(jax.random.fold_in(key_list[14], 71), 0)
    key_second = draw_key_second(jax.random.fold_in(key_list[14], 71), 0)
    value_weight = gaussian(key_list[9], (D, HEADS * VALUE_DIM), D ** -0.5, 0.125, ((1, 8),))
    lambda_head = jnp.clip(0.3 + 0.5 * jax.random.uniform(key_list[10], (HEADS,), jnp.float32) ** shard_levels(key_list[10], (HEADS,), ((0, 8),), -0.2, 0.2), 0.3, 0.8)
    context_score_boost = jnp.clip(1.5 + 1.5 * jax.random.uniform(key_list[11], (HEADS,), jnp.float32) ** shard_levels(key_list[11], (HEADS,), ((0, 8),), -0.2, 0.2), 1.5, 3.0)
    head_gain = jnp.clip(1.0 + 0.18 * jax.random.normal(key_list[12], (VALUE_DIM,), jnp.float32), 0.1, 1.9)
    output_weight = gaussian(key_list[13], (HEADS * VALUE_DIM, D), (HEADS * VALUE_DIM) ** -0.5, 0.1875, ((0, 8),))
    return {"latent": latent, "context": context, "condition": condition, "context_condition": context_condition, "modulation_weight": modulation_weight, "query_first": query_first, "query_second": query_second, "key_first": key_first, "key_second": key_second, "value_weight": value_weight, "lambda_head": lambda_head, "context_score_boost": context_score_boost, "head_gain": head_gain, "output_weight": output_weight}


EPSILON = 1e-06
THETA = 10000.0

def norm_rows(rows):
    values = rows.astype(jnp.float32)
    return values * lax.rsqrt(lax.optimization_barrier(jnp.mean(values * values, axis=-1, keepdims=True)) + EPSILON)

def rotate_pairs(values, positions):
    half = values.shape[-1] // 2
    quarter = half // 2
    reciprocal_norm = THETA ** (-jnp.arange(quarter, dtype=jnp.float32) / quarter)

    def turn(part, where):
        angle = where.astype(jnp.float32)[:, None] * reciprocal_norm[None, :]
        cosine_table = jnp.concatenate([jnp.cos(angle)] * 2, -1)[:, None, :]
        sine = jnp.concatenate([jnp.sin(angle)] * 2, -1)[:, None, :]
        flipped = jnp.concatenate([-part[..., quarter:], part[..., :quarter]], -1)
        return part * cosine_table + flipped * sine
    grid_row = positions // GRID_W
    grid_col = positions % GRID_W
    return jnp.concatenate([turn(values[..., :half], grid_row), turn(values[..., half:], grid_col)], -1)

def project(rows, weight):
    return jnp.dot(rows, weight, preferred_element_type=jnp.float32).reshape(rows.shape[0], HEADS, -1)

def reference(latent, context, condition, context_condition, modulation_weight, query_first, query_second, key_first, key_second, value_weight, lambda_head, context_score_boost, head_gain, output_weight):
    signal = jax.nn.silu(jnp.stack([condition, context_condition])).astype(jnp.bfloat16)
    modulation = jnp.dot(signal, modulation_weight, preferred_element_type=jnp.float32)
    shift = modulation[:, :D]
    scale = modulation[:, D:2 * D]
    gate = modulation[:, 2 * D:]
    h_latent = (norm_rows(latent) * (1.0 + scale[0]) + shift[0]).astype(jnp.bfloat16)
    h_context = (norm_rows(context) * (1.0 + scale[1]) + shift[1]).astype(jnp.bfloat16)
    positions = jnp.arange(TOKENS, dtype=jnp.int32)
    queries_one = rotate_pairs(project(h_latent, query_first), positions).astype(jnp.bfloat16)
    queries_two = rotate_pairs(project(h_latent, query_second), positions).astype(jnp.bfloat16)
    latent_one = rotate_pairs(project(h_latent, key_first), positions).astype(jnp.bfloat16)
    latent_two = rotate_pairs(project(h_latent, key_second), positions).astype(jnp.bfloat16)
    latent_values = project(h_latent, value_weight).astype(jnp.bfloat16)
    context_one = project(h_context, key_first).astype(jnp.bfloat16)
    context_two = project(h_context, key_second).astype(jnp.bfloat16)
    context_values = project(h_context, value_weight).astype(jnp.bfloat16)
    keys_one = jnp.concatenate([context_one, latent_one], 0).astype(jnp.float32)
    keys_two = jnp.concatenate([context_two, latent_two], 0).astype(jnp.float32)
    values_all = jnp.concatenate([context_values, latent_values], 0).astype(jnp.float32)
    lift = jnp.concatenate([jnp.broadcast_to(context_score_boost[:, None], (HEADS, CTX)), jnp.zeros((HEADS, TOKENS), jnp.float32)], 1)[:, None, :]
    block = 256 if TOKENS % 256 == 0 else TOKENS
    count = TOKENS // block

    def attend(pair):
        query_one, query_two = pair
        outcomes = []
        for query, keys in ((query_one, keys_one), (query_two, keys_two)):
            scores = jnp.einsum('qhd,khd->hqk', query.astype(jnp.float32), keys) * HEAD_DIM ** (-0.5) + lift
            highest = lax.optimization_barrier(jnp.max(scores, axis=-1, keepdims=True))
            exp_weights = jnp.exp(scores - highest)
            totals = lax.optimization_barrier(jnp.sum(exp_weights, axis=-1))
            rounded = lax.optimization_barrier(exp_weights.astype(jnp.bfloat16))
            weighted = jnp.einsum('hqk,khe->qhe', rounded.astype(jnp.float32), values_all)
            outcomes.append(weighted / jnp.transpose(totals)[:, :, None])
        return outcomes[0] - lambda_head[None, :, None] * outcomes[1]
    blocks = (queries_one.reshape(count, block, HEADS, HEAD_DIM), queries_two.reshape(count, block, HEADS, HEAD_DIM))
    mixed = lax.map(attend, blocks).reshape(TOKENS, HEADS, VALUE_DIM)
    normed = mixed * lax.rsqrt(lax.optimization_barrier(jnp.mean(mixed * mixed, axis=-1, keepdims=True)) + EPSILON) * head_gain
    heads_out = normed.astype(jnp.bfloat16).reshape(TOKENS, HEADS * VALUE_DIM)
    branch = jnp.dot(heads_out, output_weight, preferred_element_type=jnp.float32)
    return (latent.astype(jnp.float32) + gate[0] * branch).astype(jnp.bfloat16)
```

```python
import functools
import math

import jax
import jax.numpy as jnp
import numpy as np
from jax import lax
from jax.experimental import pallas as pl
from jax.experimental.pallas import tpu as pltpu
from jax.sharding import PartitionSpec as P

MESH = pl.DeviceIdType.MESH
EPSILON = 1e-06
THETA = 10000.0
GRID_W = 64
RING = 8
TP = 8
ROWS = 32
BLOCK = 256
CTX = 8
KEYS = BLOCK + 2 * CTX
WIDTH = 2048
CHUNK = 96
LOG2E = math.log2(math.e)
BF16 = jnp.bfloat16
F32 = jnp.float32

NT = (((1,), (1,)), ((), ()))
NN = (((1,), (0,)), ((), ()))


def dot(a, b, dims=NN):
    return lax.dot_general(a, b, dims, preferred_element_type=F32)


def remote(src, dst, send, recv, sp, tp):
    return pltpu.make_async_remote_copy(
        src_ref=src, dst_ref=dst, send_sem=send, recv_sem=recv, device_id=(sp, tp), device_id_type=MESH
    )


def silu(v):
    return v / (1.0 + jnp.exp(-v))


def kernel(
    latent, context, cond, ccond, modw, wq1, wq2, wk1, wk2, wv, lam, boost, gain, wout, freq,
    out,
    lat, ctx, mw, w64, wcat, wo, part, modg, modv, h, cosb, sinb, qb, kvb, vx, kc,
    osend, ssend, orecv, srecv, hsend, hrecv,
    load, part_s, part_r, y_s, y_r, z_s, z_r, lat_s, lat_r, latf_s, wo_s, wo_r, wof_s,
    q_s, q_r, kv_s, kv_r, o_s, o_r, st_s, st_r, h_s, h_r,
):
    sp, tp = lax.axis_index("sp"), lax.axis_index("tp")
    z, y = sp // RING, sp % RING
    x, core = tp // 2, tp % 2
    partner = x * 2 + 1 - core
    a = core * z + (1 - core) * y
    b = core * y + (1 - core) * z

    def at_a(i):
        return (1 - core) * (z * RING + i) + core * (i * RING + y)

    def at_b(i):
        return (1 - core) * (i * RING + y) + core * (z * RING + i)

    def chip(d):
        return ((x + d) % 4) * 2 + core

    loads = [
        pltpu.make_async_copy(modw, mw, load.at[0]),
        pltpu.make_async_copy(latent, lat.at[tp], load.at[1]),
        pltpu.make_async_copy(context, ctx, load.at[2]),
        pltpu.make_async_copy(wout, wo.at[tp], load.at[3]),
        pltpu.make_async_copy(wq1, w64.at[0], load.at[4]),
        pltpu.make_async_copy(wq2, w64.at[1], load.at[5]),
        pltpu.make_async_copy(wk1, w64.at[2], load.at[6]),
        pltpu.make_async_copy(wk2, w64.at[3], load.at[7]),
        pltpu.make_async_copy(wv, wcat.at[:, 256:384], load.at[8]),
    ]
    for c in loads:
        c.start()

    barrier = pltpu.get_barrier_semaphore()
    for d in range(1, TP):
        pl.semaphore_signal(barrier, inc=1, device_id=(sp, (tp + d) % TP), device_id_type=MESH)
    for d in range(1, RING):
        pl.semaphore_signal(barrier, inc=1, device_id=(at_a((a + d) % RING), tp), device_id_type=MESH)
        pl.semaphore_signal(barrier, inc=1, device_id=(at_b((b + d) % RING), tp), device_id_type=MESH)

    loads[0].wait()
    signal = silu(jnp.concatenate([cond[...], ccond[...], jnp.zeros((6, 256), F32)], axis=0)).astype(BF16)
    mine = dot(signal, mw[...])[0:2]
    part[0] = jnp.concatenate([mine, jnp.zeros((2, 128 - CHUNK), F32)], axis=1)
    loads[1].wait()
    loads[3].wait()
    pl.semaphore_wait(barrier, TP - 1 + 2 * (RING - 1))

    parts = [
        remote(part.at[0], part.at[d], part_s.at[d], part_r.at[d], sp, (tp + d) % TP) for d in range(1, TP)
    ]
    for c in parts:
        c.start()
    lats = [remote(lat.at[tp], lat.at[tp], lat_s.at[d], lat_r.at[tp], sp, chip(d)) for d in range(1, 4)]
    lats.append(remote(lat.at[tp], lat.at[tp], lat_s.at[0], lat_r.at[tp], sp, partner))
    for c in lats:
        c.start()
    wos = [remote(wo.at[tp], wo.at[tp], wo_s.at[d], wo_r.at[tp], sp, chip(d)) for d in range(1, 4)]
    wos.append(remote(wo.at[tp], wo.at[tp], wo_s.at[0], wo_r.at[tp], sp, partner))
    for c in wos:
        c.start()

    for c in parts:
        c.wait_recv()
    total = part[0]
    for d in range(1, TP):
        total = total + part[d]
    modg[z, y] = total
    ys = [
        remote(modg.at[z, y], modg.at[z, y], y_s.at[d], y_r.at[y], z * RING + (y + d) % RING, tp)
        for d in range(1, RING)
    ]
    for c in ys:
        c.start()

    row = lax.broadcasted_iota(jnp.int32, (BLOCK, 128), 0)
    lane = lax.broadcasted_iota(jnp.int32, (BLOCK, 128), 1)
    token = row + sp * BLOCK
    grid_row = token // GRID_W
    where = jnp.where(lane % 64 < 32, grid_row, token - grid_row * GRID_W).astype(F32)
    angle = where * freq[...]
    cosb[...] = jnp.cos(angle)
    sinb[...] = jnp.where(lane % 32 < 16, -jnp.sin(angle), jnp.sin(angle))

    for d in range(1, RING):
        other = (y + d) % RING
        remote(modg.at[z, other], modg.at[z, other], y_s.at[0], y_r.at[other], sp, tp).wait_recv()
    zs = [
        remote(modg.at[z], modg.at[z], z_s.at[d], z_r.at[z], ((z + d) % RING) * RING + y, tp)
        for d in range(1, RING)
    ]
    for c in zs:
        c.start()

    for c in loads[4:]:
        c.wait()
    wcat[:, 0:128] = jnp.concatenate([w64[0], w64[1]], axis=1)
    wcat[:, 128:256] = jnp.concatenate([w64[2], w64[3]], axis=1)
    ones = jnp.ones((BLOCK, 128), BF16)
    for j in range(RING):
        vx[j, :, 128:256] = ones
    vx[RING, :, 128:256] = ones
    fwd = []
    for d in range(1, 4):
        slot = chip(d)
        remote(lat.at[slot], lat.at[slot], lat_s.at[d], lat_r.at[slot], sp, tp).wait_recv()
        c = remote(lat.at[slot], lat.at[slot], latf_s.at[d], lat_r.at[slot], sp, partner)
        c.start()
        fwd.append(c)

    for d in range(1, RING):
        other = (z + d) % RING
        remote(modg.at[other], modg.at[other], z_s.at[0], z_r.at[other], sp, tp).wait_recv()

    lane2 = lax.broadcasted_iota(jnp.int32, (2, 128), 1)
    for g in range(16):
        c0, c1, c2, c3 = [modg[g // 2, (g % 2) * 4 + j] for j in range(4)]
        c1, c2, c3 = pltpu.roll(c1, 96, 1), pltpu.roll(c2, 64, 1), pltpu.roll(c3, 32, 1)
        rows = [jnp.where(lane2 < 96, c0, c1), jnp.where(lane2 < 64, c1, c2), jnp.where(lane2 < 32, c2, c3)]
        for m in range(3):
            for r in range(2):
                modv[r, 3 * g + m : 3 * g + m + 1, :] = rows[m][r : r + 1]

    loads[2].wait()

    def modulated(v, r):
        scaled = v * lax.rsqrt(jnp.mean(v * v, axis=1, keepdims=True) + EPSILON)
        pieces = []
        for k in range(WIDTH // 128):
            piece = scaled[:, k * 128 : (k + 1) * 128]
            piece = piece * (1.0 + modv[r, 16 + k : 17 + k, :]) + modv[r, k : k + 1, :]
            pieces.append(piece)
        return jnp.concatenate(pieces, axis=1)

    hc = modulated(ctx[...].astype(F32), 1)
    h[BLOCK:KEYS, :] = jnp.concatenate([hc, jnp.zeros((CTX, WIDTH), F32)], axis=0).astype(BF16)

    for d in range(4):
        slot = ((x + d) % 4) * 2 + 1 - core
        remote(lat.at[slot], lat.at[slot], lat_s.at[0], lat_r.at[slot], sp, tp).wait_recv()

    def fill(i, carry):
        v = lat[i // 2, pl.ds(pl.multiple_of((i % 2) * 16, 16), 16), :].astype(F32)
        h[pl.ds(pl.multiple_of(i * 16, 16), 16), :] = modulated(v, 0).astype(BF16)
        return carry

    lax.fori_loop(0, BLOCK // 16, fill, 0)

    qkv = dot(h[...], wcat[...])
    cosine, sine = cosb[...], sinb[...]

    def rope(v):
        turned = jnp.where(lane % 32 < 16, pltpu.roll(v, 112, 1), pltpu.roll(v, 16, 1))
        return v * cosine + turned * sine

    qb[0] = (rope(qkv[0:BLOCK, 0:128]) * (LOG2E / 8.0)).astype(BF16)
    kvb[0, 0:BLOCK, 0:128] = rope(qkv[0:BLOCK, 128:256]).astype(BF16)
    kvb[0, BLOCK:KEYS, 0:128] = qkv[BLOCK:KEYS, 128:256].astype(BF16)
    kvb[0, :, 128:256] = qkv[:, 256:384].astype(BF16)

    kvs = [
        remote(kvb.at[0], kvb.at[d], kv_s.at[d], kv_r.at[d], at_b((b + d) % RING), tp) for d in range(1, RING)
    ]
    qs = [remote(qb.at[0], qb.at[d], q_s.at[d], q_r.at[d], at_a((a + d) % RING), tp) for d in range(1, RING)]
    for i in (0, 6, 1, 5, 2, 4, 3):
        qs[i].start()
        kvs[i].start()
    for i in (0, 6, 1, 5, 2, 4, 3):
        qs[i].wait_recv()
        kvs[i].wait_recv()

    for j in range(RING):
        vx[j, :, 0:128] = kvb[j, 0:BLOCK, 128:256]
        kc[j * 16 : (j + 1) * 16, :] = kvb[j, BLOCK:KEYS, 0:128]
        vx[RING, j * 16 : (j + 1) * 16, 0:128] = kvb[j, BLOCK:KEYS, 128:256]
    lane1 = lax.broadcasted_iota(jnp.int32, (1, 128), 1)
    bias = jnp.where(lane1 % 16 < CTX, boost[0] * LOG2E, -1e30)
    laneq = lax.broadcasted_iota(jnp.int32, (BLOCK, 128), 1)

    def attend(query):
        scores = [dot(query, kvb[j, 0:BLOCK, 0:128], NT) for j in range(RING)]
        extra = dot(query, kc[...], NT) + bias
        peak = scores[0]
        for s in scores[1:]:
            peak = jnp.maximum(peak, s)
        peak = jnp.maximum(jnp.maximum(peak[:, 0:128], peak[:, 128:256]), extra)
        peak = jnp.max(peak, axis=1, keepdims=True)
        acc = dot(jnp.exp2(extra - peak).astype(BF16), vx[RING, 0:128, :])
        for j in range(RING):
            acc = acc + dot(jnp.exp2(scores[j] - peak).astype(BF16), vx[j])
        sums = acc[:, 128:256]
        return (acc[:, 0:128] / sums).astype(BF16), peak + jnp.log2(sums)

    def block(k):
        d = (4 + ((k + 1) // 2) * (1 - 2 * (k % 2))) % RING
        query = qb[d]
        none = jnp.zeros_like(query)
        one, level_one = attend(jnp.where(laneq < 64, query, none))
        two, level_two = attend(jnp.where(laneq < 64, none, query))
        osend[k, :, 0:128] = one
        osend[k, :, 128:256] = two
        levels = jnp.where(laneq % 8 < 4, level_one, level_two)
        ssend[k] = jnp.transpose(levels)[0:8, :]
        return d

    def back(k, carry):
        d = block(k)
        to = at_a((a - d + RING) % RING)
        remote(ssend.at[k], srecv.at[d], st_s.at[k], st_r.at[d], to, tp).start()
        remote(osend.at[k], orecv.at[d], o_s.at[k], o_r.at[d], to, tp).start()
        return carry

    lax.fori_loop(0, 4, back, 0)
    wofwd = []
    for d in range(1, 4):
        slot = chip(d)
        remote(wo.at[slot], wo.at[slot], wo_s.at[d], wo_r.at[slot], sp, tp).wait_recv()
        c = remote(wo.at[slot], wo.at[slot], wof_s.at[d], wo_r.at[slot], sp, partner)
        c.start()
        wofwd.append(c)
    lax.fori_loop(4, RING - 1, back, 0)
    block(RING - 1)

    for d in range(1, RING):
        remote(ssend.at[0], srecv.at[d], st_s.at[0], st_r.at[d], sp, tp).wait_recv()
    levels = [ssend[RING - 1]] + [srecv[d] for d in range(1, RING)]
    peak = levels[0]
    for v in levels[1:]:
        peak = jnp.maximum(peak, v)
    shares = [jnp.exp2(v - peak) for v in levels]
    sums = shares[0]
    for v in shares[1:]:
        sums = sums + v
    half = lax.broadcasted_iota(jnp.int32, (8, BLOCK), 0) < 4
    factor = jnp.where(half, 1.0, -lam[0]) / sums
    weights = jnp.transpose(jnp.concatenate([v * factor for v in shares] * 2, axis=0))
    for d in range(1, RING):
        remote(osend.at[0], orecv.at[d], o_s.at[0], o_r.at[d], sp, tp).wait_recv()
    mixed = jnp.zeros((BLOCK, 128), F32)
    for d in range(RING):
        u = (osend[RING - 1] if d == 0 else orecv[d]).astype(F32)
        mixed = mixed + u[:, 0:128] * weights[:, 8 * d : 8 * d + 1]
        mixed = mixed + u[:, 128:256] * weights[:, 8 * d + 4 : 8 * d + 5]
    normed = mixed * lax.rsqrt(jnp.mean(mixed * mixed, axis=1, keepdims=True) + EPSILON) * gain[...]
    hsend[...] = normed.astype(BF16).reshape(TP, ROWS, 128)
    hs = [
        remote(hsend.at[(tp + d) % TP], hrecv.at[tp], h_s.at[d], h_r.at[tp], sp, (tp + d) % TP)
        for d in range(1, TP)
    ]
    for c in hs:
        c.start()
    hrecv[tp] = hsend[tp]
    for d in range(4):
        slot = ((x + d) % 4) * 2 + 1 - core
        remote(wo.at[slot], wo.at[slot], wo_s.at[0], wo_r.at[slot], sp, tp).wait_recv()
    for d in range(1, TP):
        slot = (tp + d) % TP
        remote(hrecv.at[slot], hrecv.at[slot], h_s.at[0], h_r.at[slot], sp, tp).wait_recv()
    heads = jnp.concatenate([hrecv[j] for j in range(TP)], axis=1)
    for k in range(WIDTH // 256):
        cols = slice(k * 256, (k + 1) * 256)
        branch = dot(heads, wo[:, :, cols].reshape(TP * 128, 256))
        gate = jnp.concatenate([modv[0, 32 + 2 * k : 33 + 2 * k, :], modv[0, 33 + 2 * k : 34 + 2 * k, :]], axis=1)
        out[:, cols] = (lat[tp, :, cols].astype(F32) + gate * branch).astype(BF16)

    for c in parts + lats + wos + ys + zs + fwd + wofwd + qs + kvs + hs:
        c.wait_send()
    for k in range(RING - 1):
        remote(ssend.at[k], srecv.at[k], st_s.at[k], st_r.at[k], sp, tp).wait_send()
        remote(osend.at[k], orecv.at[k], o_s.at[k], o_r.at[k], sp, tp).wait_send()


def body(
    latent, context, condition, context_condition, modulation_weight, query_first, query_second, key_first,
    key_second, value_weight, lambda_head, context_score_boost, head_gain, output_weight,
):
    freq = jnp.asarray(np.tile(THETA ** (-np.arange(16, dtype=np.float32) / 16), 8)[None].astype(np.float32))
    vmem = pl.BlockSpec(memory_space=pltpu.VMEM)
    smem = pl.BlockSpec(memory_space=pltpu.SMEM)
    hbm = pl.BlockSpec(memory_space=pl.ANY)
    dma = pltpu.SemaphoreType.DMA
    return pl.pallas_call(
        kernel,
        out_shape=jax.ShapeDtypeStruct((ROWS, WIDTH), BF16),
        in_specs=[hbm, hbm, vmem, vmem, hbm, hbm, hbm, hbm, hbm, hbm, smem, smem, vmem, hbm, vmem],
        out_specs=vmem,
        scratch_shapes=[
            pltpu.VMEM((TP, ROWS, WIDTH), BF16),
            pltpu.VMEM((CTX, WIDTH), BF16),
            pltpu.VMEM((256, CHUNK), BF16),
            pltpu.VMEM((4, WIDTH, 64), BF16),
            pltpu.VMEM((WIDTH, 384), BF16),
            pltpu.VMEM((TP, 128, WIDTH), BF16),
            pltpu.VMEM((TP, 2, 128), F32),
            pltpu.VMEM((RING, RING, 2, 128), F32),
            pltpu.VMEM((2, 48, 128), F32),
            pltpu.VMEM((KEYS, WIDTH), BF16),
            pltpu.VMEM((BLOCK, 128), F32),
            pltpu.VMEM((BLOCK, 128), F32),
            pltpu.VMEM((RING, BLOCK, 128), BF16),
            pltpu.VMEM((RING, KEYS, 256), BF16),
            pltpu.VMEM((RING + 1, BLOCK, 256), BF16),
            pltpu.VMEM((128, 128), BF16),
            pltpu.VMEM((RING, BLOCK, 256), BF16),
            pltpu.VMEM((RING, 8, BLOCK), F32),
            pltpu.VMEM((RING, BLOCK, 256), BF16),
            pltpu.VMEM((RING, 8, BLOCK), F32),
            pltpu.VMEM((TP, ROWS, 128), BF16),
            pltpu.VMEM((TP, ROWS, 128), BF16),
            dma((9,)),
            dma((8,)), dma((8,)), dma((8,)), dma((8,)), dma((8,)), dma((8,)),
            dma((4,)), dma((8,)), dma((4,)), dma((4,)), dma((8,)), dma((4,)),
            dma((8,)), dma((8,)), dma((8,)), dma((8,)), dma((8,)), dma((8,)),
            dma((8,)), dma((8,)), dma((8,)), dma((8,)),
        ],
        compiler_params=pltpu.CompilerParams(
            collective_id=0, has_side_effects=True, vmem_limit_bytes=60 * 2**20
        ),
        name="whole",
    )(
        latent, context, condition.reshape(1, 256), context_condition.reshape(1, 256), modulation_weight,
        query_first, query_second, key_first, key_second, value_weight, lambda_head, context_score_boost,
        head_gain.reshape(1, 128), output_weight, freq,
    )


def solution(mesh):
    in_specs = (
        P(("sp", "tp"), None), P("sp", None), P("tp"), P("tp"), P("tp", "sp"), P(None, "tp"), P(None, "tp"),
        P(None, "tp"), P(None, "tp"), P(None, "tp"), P("tp"), P("tp"), P(), P("tp", None),
    )
    out_specs = P(("sp", "tp"), None)
    return jax.shard_map(body, mesh=mesh, in_specs=in_specs, out_specs=out_specs, check_vma=False)
```

```python
import functools
import math

import jax
import jax.numpy as jnp
import numpy as np
from jax import lax
from jax.experimental import pallas as pl
from jax.experimental.pallas import tpu as pltpu
from jax.sharding import PartitionSpec as P

MESH = pl.DeviceIdType.MESH
EPSILON = 1e-06
THETA = 10000.0
GRID_W = 64
RING = 8
TP = 8
ROWS = 32
BLOCK = 256
CTX = 8
KEYS = BLOCK + 2 * CTX
WIDTH = 2048
CHUNK = 96
LOG2E = math.log2(math.e)
BF16 = jnp.bfloat16
F32 = jnp.float32

NT = (((1,), (1,)), ((), ()))
NN = (((1,), (0,)), ((), ()))


def dot(a, b, dims=NN):
    return lax.dot_general(a, b, dims, preferred_element_type=F32)


def remote(src, dst, send, recv, sp, tp):
    return pltpu.make_async_remote_copy(
        src_ref=src, dst_ref=dst, send_sem=send, recv_sem=recv, device_id=(sp, tp), device_id_type=MESH
    )


def silu(v):
    return v / (1.0 + jnp.exp(-v))


def kernel(
    latent, context, cond, ccond, modw, wq1, wq2, wk1, wk2, wv, lam, boost, gain, wout, freq,
    out,
    lat, ctx, mw, wqk, wval, wo, part, modg, modv, h, cosb, sinb, qb, kvb, vx, kc,
    osend, ssend, orecv, srecv, hsend, hrecv,
    load, part_s, part_r, y_s, y_r, z_s, z_r, lat_s, lat_r, latf_s, wo_s, wo_r, wof_s,
    q_s, q_r, kv_s, kv_r, o_s, o_r, st_s, st_r, h_s, h_r,
):
    sp, tp = lax.axis_index("sp"), lax.axis_index("tp")
    z, y = sp // RING, sp % RING
    x, core = tp // 2, tp % 2
    partner = x * 2 + 1 - core
    a = core * z + (1 - core) * y
    b = core * y + (1 - core) * z

    def at_a(i):
        return (1 - core) * (z * RING + i) + core * (i * RING + y)

    def at_b(i):
        return (1 - core) * (i * RING + y) + core * (z * RING + i)

    def chip(d):
        return ((x + d) % 4) * 2 + core

    loads = [
        pltpu.make_async_copy(modw, mw, load.at[0]),
        pltpu.make_async_copy(latent, lat.at[tp], load.at[1]),
        pltpu.make_async_copy(context, ctx, load.at[2]),
        pltpu.make_async_copy(wout, wo.at[tp], load.at[3]),
        pltpu.make_async_copy(wq1, wqk.at[0:64], load.at[4]),
        pltpu.make_async_copy(wq2, wqk.at[64:128], load.at[5]),
        pltpu.make_async_copy(wk1, wqk.at[128:192], load.at[6]),
        pltpu.make_async_copy(wk2, wqk.at[192:256], load.at[7]),
        pltpu.make_async_copy(wv, wval, load.at[8]),
    ]
    for c in loads:
        c.start()

    barrier = pltpu.get_barrier_semaphore()
    for d in range(1, TP):
        pl.semaphore_signal(barrier, inc=1, device_id=(sp, (tp + d) % TP), device_id_type=MESH)
    for d in range(1, RING):
        pl.semaphore_signal(barrier, inc=1, device_id=(at_a((a + d) % RING), tp), device_id_type=MESH)
        pl.semaphore_signal(barrier, inc=1, device_id=(at_b((b + d) % RING), tp), device_id_type=MESH)

    loads[0].wait()
    signal = silu(jnp.concatenate([cond[...], ccond[...], jnp.zeros((6, 256), F32)], axis=0)).astype(BF16)
    mine = dot(signal, mw[...], NT)[0:2]
    part[0] = jnp.concatenate([mine, jnp.zeros((2, 128 - CHUNK), F32)], axis=1)
    loads[1].wait()
    loads[3].wait()
    pl.semaphore_wait(barrier, TP - 1 + 2 * (RING - 1))

    parts = [
        remote(part.at[0], part.at[d], part_s.at[d], part_r.at[d], sp, (tp + d) % TP) for d in range(1, TP)
    ]
    for c in parts:
        c.start()
    lats = [remote(lat.at[tp], lat.at[tp], lat_s.at[d], lat_r.at[tp], sp, chip(d)) for d in range(1, 4)]
    lats.append(remote(lat.at[tp], lat.at[tp], lat_s.at[0], lat_r.at[tp], sp, partner))
    for c in lats:
        c.start()

    for c in parts:
        c.wait_recv()
    total = part[0]
    for d in range(1, TP):
        total = total + part[d]
    modg[z, y] = total
    ys = [
        remote(modg.at[z, y], modg.at[z, y], y_s.at[d], y_r.at[y], z * RING + (y + d) % RING, tp)
        for d in range(1, RING)
    ]
    for c in ys:
        c.start()

    row = lax.broadcasted_iota(jnp.int32, (BLOCK, 128), 0)
    lane = lax.broadcasted_iota(jnp.int32, (BLOCK, 128), 1)
    token = row + sp * BLOCK
    grid_row = token // GRID_W
    where = jnp.where(lane % 64 < 32, grid_row, token - grid_row * GRID_W).astype(F32)
    angle = where * freq[...]
    cosb[...] = jnp.cos(angle)
    sinb[...] = jnp.where(lane % 32 < 16, -jnp.sin(angle), jnp.sin(angle))

    for d in range(1, RING):
        other = (y + d) % RING
        remote(modg.at[z, other], modg.at[z, other], y_s.at[0], y_r.at[other], sp, tp).wait_recv()
    zs = [
        remote(modg.at[z], modg.at[z], z_s.at[d], z_r.at[z], ((z + d) % RING) * RING + y, tp)
        for d in range(1, RING)
    ]
    for c in zs:
        c.start()

    for c in loads[4:]:
        c.wait()
    ones = jnp.ones((BLOCK, 128), BF16)
    for j in range(RING):
        vx[j, :, 128:256] = ones
    vx[RING, :, 128:256] = ones
    fwd = []
    for d in range(1, 4):
        slot = chip(d)
        remote(lat.at[slot], lat.at[slot], lat_s.at[d], lat_r.at[slot], sp, tp).wait_recv()
        c = remote(lat.at[slot], lat.at[slot], latf_s.at[d], lat_r.at[slot], sp, partner)
        c.start()
        fwd.append(c)

    for d in range(1, RING):
        other = (z + d) % RING
        remote(modg.at[other], modg.at[other], z_s.at[0], z_r.at[other], sp, tp).wait_recv()

    lane2 = lax.broadcasted_iota(jnp.int32, (2, 128), 1)
    for g in range(16):
        c0, c1, c2, c3 = [modg[g // 2, (g % 2) * 4 + j] for j in range(4)]
        c1, c2, c3 = pltpu.roll(c1, 96, 1), pltpu.roll(c2, 64, 1), pltpu.roll(c3, 32, 1)
        rows = [jnp.where(lane2 < 96, c0, c1), jnp.where(lane2 < 64, c1, c2), jnp.where(lane2 < 32, c2, c3)]
        for m in range(3):
            for r in range(2):
                modv[r, 3 * g + m : 3 * g + m + 1, :] = rows[m][r : r + 1]

    loads[2].wait()

    def modulated(v, r):
        scaled = v * lax.rsqrt(jnp.mean(v * v, axis=1, keepdims=True) + EPSILON)
        pieces = []
        for k in range(WIDTH // 128):
            piece = scaled[:, k * 128 : (k + 1) * 128]
            piece = piece * (1.0 + modv[r, 16 + k : 17 + k, :]) + modv[r, k : k + 1, :]
            pieces.append(piece)
        return jnp.concatenate(pieces, axis=1)

    hc = modulated(ctx[...].astype(F32), 1)
    h[BLOCK:KEYS, :] = jnp.concatenate([hc, jnp.zeros((CTX, WIDTH), F32)], axis=0).astype(BF16)

    for d in range(4):
        slot = ((x + d) % 4) * 2 + 1 - core
        remote(lat.at[slot], lat.at[slot], lat_s.at[0], lat_r.at[slot], sp, tp).wait_recv()

    wos = [remote(wo.at[tp], wo.at[tp], wo_s.at[d], wo_r.at[tp], sp, chip(d)) for d in range(1, 4)]
    wos.append(remote(wo.at[tp], wo.at[tp], wo_s.at[0], wo_r.at[tp], sp, partner))
    for c in wos:
        c.start()
    def fill(i, carry):
        v = lat[i // 2, pl.ds(pl.multiple_of((i % 2) * 16, 16), 16), :].astype(F32)
        h[pl.ds(pl.multiple_of(i * 16, 16), 16), :] = modulated(v, 0).astype(BF16)
        return carry

    lax.fori_loop(0, BLOCK // 16, fill, 0)

    qk = dot(h[...], wqk[...], NT)
    val = dot(h[...], wval[...])
    cosine, sine = cosb[...], sinb[...]

    def rope(v):
        turned = jnp.where(lane % 32 < 16, pltpu.roll(v, 112, 1), pltpu.roll(v, 16, 1))
        return v * cosine + turned * sine

    qb[0] = (rope(qk[0:BLOCK, 0:128]) * (LOG2E / 8.0)).astype(BF16)
    kvb[0, 0:BLOCK, 0:128] = rope(qk[0:BLOCK, 128:256]).astype(BF16)
    kvb[0, BLOCK:KEYS, 0:128] = qk[BLOCK:KEYS, 128:256].astype(BF16)
    kvb[0, :, 128:256] = val.astype(BF16)

    kvs = [
        remote(kvb.at[0], kvb.at[d], kv_s.at[d], kv_r.at[d], at_b((b + d) % RING), tp) for d in range(1, RING)
    ]
    qs = [remote(qb.at[0], qb.at[d], q_s.at[d], q_r.at[d], at_a((a + d) % RING), tp) for d in range(1, RING)]
    for i in (0, 6, 1, 5, 2, 4, 3):
        qs[i].start()
        kvs[i].start()
    for i in (0, 6, 1, 5, 2, 4, 3):
        qs[i].wait_recv()
        kvs[i].wait_recv()

    for j in range(RING):
        vx[j, :, 0:128] = kvb[j, 0:BLOCK, 128:256]
        kc[j * 16 : (j + 1) * 16, :] = kvb[j, BLOCK:KEYS, 0:128]
        vx[RING, j * 16 : (j + 1) * 16, 0:128] = kvb[j, BLOCK:KEYS, 128:256]
    lane1 = lax.broadcasted_iota(jnp.int32, (1, 128), 1)
    bias = jnp.where(lane1 % 16 < CTX, boost[0] * LOG2E, -1e30)
    laneq = lax.broadcasted_iota(jnp.int32, (BLOCK, 128), 1)

    def attend(query):
        scores = [dot(query, kvb[j, 0:BLOCK, 0:128], NT) for j in range(RING)]
        extra = dot(query, kc[...], NT) + bias
        peak = scores[0]
        for s in scores[1:]:
            peak = jnp.maximum(peak, s)
        peak = jnp.maximum(jnp.maximum(peak[:, 0:128], peak[:, 128:256]), extra)
        peak = jnp.max(peak, axis=1, keepdims=True)
        acc = dot(jnp.exp2(extra - peak).astype(BF16), vx[RING, 0:128, :])
        for j in range(RING):
            acc = acc + dot(jnp.exp2(scores[j] - peak).astype(BF16), vx[j])
        sums = acc[:, 128:256]
        return (acc[:, 0:128] / sums).astype(BF16), peak + jnp.log2(sums)

    def block(k):
        d = (4 + ((k + 1) // 2) * (1 - 2 * (k % 2))) % RING
        query = qb[d]
        none = jnp.zeros_like(query)
        one, level_one = attend(jnp.where(laneq < 64, query, none))
        two, level_two = attend(jnp.where(laneq < 64, none, query))
        osend[k, :, 0:128] = one
        osend[k, :, 128:256] = two
        levels = jnp.where(laneq % 8 < 4, level_one, level_two)
        ssend[k] = jnp.transpose(levels)[0:8, :]
        return d

    def back(k, carry):
        d = block(k)
        to = at_a((a - d + RING) % RING)
        remote(ssend.at[k], srecv.at[d], st_s.at[k], st_r.at[d], to, tp).start()
        remote(osend.at[k], orecv.at[d], o_s.at[k], o_r.at[d], to, tp).start()
        return carry

    lax.fori_loop(0, 4, back, 0)
    wofwd = []
    for d in range(1, 4):
        slot = chip(d)
        remote(wo.at[slot], wo.at[slot], wo_s.at[d], wo_r.at[slot], sp, tp).wait_recv()
        c = remote(wo.at[slot], wo.at[slot], wof_s.at[d], wo_r.at[slot], sp, partner)
        c.start()
        wofwd.append(c)
    lax.fori_loop(4, RING - 1, back, 0)
    block(RING - 1)

    for d in range(1, RING):
        remote(ssend.at[0], srecv.at[d], st_s.at[0], st_r.at[d], sp, tp).wait_recv()
    levels = [ssend[RING - 1]] + [srecv[d] for d in range(1, RING)]
    peak = levels[0]
    for v in levels[1:]:
        peak = jnp.maximum(peak, v)
    shares = [jnp.exp2(v - peak) for v in levels]
    sums = shares[0]
    for v in shares[1:]:
        sums = sums + v
    half = lax.broadcasted_iota(jnp.int32, (8, BLOCK), 0) < 4
    factor = jnp.where(half, 1.0, -lam[0]) / sums
    weights = jnp.transpose(jnp.concatenate([v * factor for v in shares] * 2, axis=0))
    for d in range(1, RING):
        remote(osend.at[0], orecv.at[d], o_s.at[0], o_r.at[d], sp, tp).wait_recv()
    mixed = jnp.zeros((BLOCK, 128), F32)
    for d in range(RING):
        u = (osend[RING - 1] if d == 0 else orecv[d]).astype(F32)
        mixed = mixed + u[:, 0:128] * weights[:, 8 * d : 8 * d + 1]
        mixed = mixed + u[:, 128:256] * weights[:, 8 * d + 4 : 8 * d + 5]
    normed = mixed * lax.rsqrt(jnp.mean(mixed * mixed, axis=1, keepdims=True) + EPSILON) * gain[...]
    hsend[...] = normed.astype(BF16).reshape(TP, ROWS, 128)
    hs = [
        remote(hsend.at[(tp + d) % TP], hrecv.at[tp], h_s.at[d], h_r.at[tp], sp, (tp + d) % TP)
        for d in range(1, TP)
    ]
    for c in hs:
        c.start()
    hrecv[tp] = hsend[tp]
    for d in range(4):
        slot = ((x + d) % 4) * 2 + 1 - core
        remote(wo.at[slot], wo.at[slot], wo_s.at[0], wo_r.at[slot], sp, tp).wait_recv()
    for d in range(1, TP):
        slot = (tp + d) % TP
        remote(hrecv.at[slot], hrecv.at[slot], h_s.at[0], h_r.at[slot], sp, tp).wait_recv()
    heads = jnp.concatenate([hrecv[j] for j in range(TP)], axis=1)
    for k in range(WIDTH // 256):
        cols = slice(k * 256, (k + 1) * 256)
        branch = dot(heads, wo[:, :, cols].reshape(TP * 128, 256))
        gate = jnp.concatenate([modv[0, 32 + 2 * k : 33 + 2 * k, :], modv[0, 33 + 2 * k : 34 + 2 * k, :]], axis=1)
        out[:, cols] = (lat[tp, :, cols].astype(F32) + gate * branch).astype(BF16)

    for c in parts + lats + wos + ys + zs + fwd + wofwd + qs + kvs + hs:
        c.wait_send()
    for k in range(RING - 1):
        remote(ssend.at[k], srecv.at[k], st_s.at[k], st_r.at[k], sp, tp).wait_send()
        remote(osend.at[k], orecv.at[k], o_s.at[k], o_r.at[k], sp, tp).wait_send()


def body(
    latent, context, condition, context_condition, modulation_weight, query_first, query_second, key_first,
    key_second, value_weight, lambda_head, context_score_boost, head_gain, output_weight,
):
    freq = jnp.asarray(np.tile(THETA ** (-np.arange(16, dtype=np.float32) / 16), 8)[None].astype(np.float32))
    vmem = pl.BlockSpec(memory_space=pltpu.VMEM)
    smem = pl.BlockSpec(memory_space=pltpu.SMEM)
    hbm = pl.BlockSpec(memory_space=pl.ANY)
    dma = pltpu.SemaphoreType.DMA
    return pl.pallas_call(
        kernel,
        out_shape=jax.ShapeDtypeStruct((ROWS, WIDTH), BF16),
        in_specs=[hbm, hbm, vmem, vmem, hbm, hbm, hbm, hbm, hbm, hbm, smem, smem, vmem, hbm, vmem],
        out_specs=vmem,
        scratch_shapes=[
            pltpu.VMEM((TP, ROWS, WIDTH), BF16),
            pltpu.VMEM((CTX, WIDTH), BF16),
            pltpu.VMEM((CHUNK, 256), BF16),
            pltpu.VMEM((256, WIDTH), BF16),
            pltpu.VMEM((WIDTH, 128), BF16),
            pltpu.VMEM((TP, 128, WIDTH), BF16),
            pltpu.VMEM((TP, 2, 128), F32),
            pltpu.VMEM((RING, RING, 2, 128), F32),
            pltpu.VMEM((2, 48, 128), F32),
            pltpu.VMEM((KEYS, WIDTH), BF16),
            pltpu.VMEM((BLOCK, 128), F32),
            pltpu.VMEM((BLOCK, 128), F32),
            pltpu.VMEM((RING, BLOCK, 128), BF16),
            pltpu.VMEM((RING, KEYS, 256), BF16),
            pltpu.VMEM((RING + 1, BLOCK, 256), BF16),
            pltpu.VMEM((128, 128), BF16),
            pltpu.VMEM((RING, BLOCK, 256), BF16),
            pltpu.VMEM((RING, 8, BLOCK), F32),
            pltpu.VMEM((RING, BLOCK, 256), BF16),
            pltpu.VMEM((RING, 8, BLOCK), F32),
            pltpu.VMEM((TP, ROWS, 128), BF16),
            pltpu.VMEM((TP, ROWS, 128), BF16),
            dma((9,)),
            dma((8,)), dma((8,)), dma((8,)), dma((8,)), dma((8,)), dma((8,)),
            dma((4,)), dma((8,)), dma((4,)), dma((4,)), dma((8,)), dma((4,)),
            dma((8,)), dma((8,)), dma((8,)), dma((8,)), dma((8,)), dma((8,)),
            dma((8,)), dma((8,)), dma((8,)), dma((8,)),
        ],
        compiler_params=pltpu.CompilerParams(
            collective_id=0, has_side_effects=True, vmem_limit_bytes=60 * 2**20
        ),
        name="whole",
    )(
        latent, context, condition.reshape(1, 256), context_condition.reshape(1, 256), modulation_weight.T,
        query_first.T, query_second.T, key_first.T, key_second.T, value_weight, lambda_head, context_score_boost,
        head_gain.reshape(1, 128), output_weight, freq,
    )


def solution(mesh):
    in_specs = (
        P(("sp", "tp"), None), P("sp", None), P("tp"), P("tp"), P("tp", "sp"), P(None, "tp"), P(None, "tp"),
        P(None, "tp"), P(None, "tp"), P(None, "tp"), P("tp"), P("tp"), P(), P("tp", None),
    )
    out_specs = P(("sp", "tp"), None)
    return jax.shard_map(body, mesh=mesh, in_specs=in_specs, out_specs=out_specs, check_vma=False)
```

```python
import functools
import math

import jax
import jax.numpy as jnp
import numpy as np
from jax import lax
from jax.experimental import pallas as pl
from jax.experimental.pallas import tpu as pltpu
from jax.sharding import PartitionSpec as P

MESH = pl.DeviceIdType.MESH
EPSILON = 1e-06
THETA = 10000.0
GRID_W = 64
RING = 8
TP = 8
ROWS = 32
BLOCK = 256
CTX = 8
KEYS = BLOCK + 2 * CTX
WIDTH = 2048
CHUNK = 96
LOG2E = math.log2(math.e)
BF16 = jnp.bfloat16
F32 = jnp.float32

NT = (((1,), (1,)), ((), ()))
NN = (((1,), (0,)), ((), ()))


def dot(a, b, dims=NN):
    return lax.dot_general(a, b, dims, preferred_element_type=F32)


def remote(src, dst, send, recv, sp, tp):
    return pltpu.make_async_remote_copy(
        src_ref=src, dst_ref=dst, send_sem=send, recv_sem=recv, device_id=(sp, tp), device_id_type=MESH
    )


def silu(v):
    return v / (1.0 + jnp.exp(-v))


def kernel(
    latent, context, cond_in, ccond_in, modw, wq1, wq2, wk1, wk2, wv, lam_in, boost_in, gain_in, wout, freq_in,
    out,
    cond, ccond, gain, freq, lam, boost, rows_out,
    lat, ctx, mw, wqk, wval, wo, part, modg, modv, nlat, nctx, cosb, sinb, qb, kb, vb, vx, kc,
    held, top, osend, ssend, orecv, srecv, hsend, hrecv,
    load, store, part_s, part_r, z_s, z_r, lat_s, lat_r, wo_s, wo_r, wo2_r,
    q_s, q_r, k_s, k_r, v_s, v_r, o_s, o_r, st_s, st_r, h_s, h_r,
):
    sp, tp = lax.axis_index("sp"), lax.axis_index("tp")
    z, y = sp // RING, sp % RING
    x, core = tp // 2, tp % 2
    partner = x * 2 + 1 - core
    a = core * z + (1 - core) * y
    b = core * y + (1 - core) * z

    def at_a(i):
        return (1 - core) * (z * RING + i) + core * (i * RING + y)

    def at_b(i):
        return (1 - core) * (i * RING + y) + core * (z * RING + i)

    def chip(d):
        return ((x + d) % 4) * 2 + core

    loads = [
        pltpu.make_async_copy(modw, mw, load.at[0]),
        pltpu.make_async_copy(latent, lat.at[tp], load.at[1]),
        pltpu.make_async_copy(context, ctx, load.at[2]),
        pltpu.make_async_copy(wout, wo.at[tp], load.at[3]),
        pltpu.make_async_copy(wq1, wqk.at[0:64], load.at[4]),
        pltpu.make_async_copy(wq2, wqk.at[64:128], load.at[5]),
        pltpu.make_async_copy(wk1, wqk.at[128:192], load.at[6]),
        pltpu.make_async_copy(wk2, wqk.at[192:256], load.at[7]),
        pltpu.make_async_copy(wv, wval, load.at[8]),
        pltpu.make_async_copy(freq_in, freq, load.at[9]),
        pltpu.make_async_copy(gain_in, gain, load.at[10]),
        pltpu.make_async_copy(lam_in, lam, load.at[11]),
        pltpu.make_async_copy(boost_in, boost, load.at[12]),
        pltpu.make_async_copy(cond_in, cond, load.at[13]),
        pltpu.make_async_copy(ccond_in, ccond, load.at[14]),
    ]
    for c in loads:
        c.start()

    barrier = pltpu.get_barrier_semaphore()

    beside = [z * RING + (y + d) % RING for d in range(RING)]
    across = [(tp + d) % TP for d in range(TP)]
    for n in range(1, TP * RING):
        pl.semaphore_signal(barrier, inc=1, device_id=(beside[n // TP], across[n % TP]), device_id_type=MESH)
    for d in range(1, RING):
        pl.semaphore_signal(barrier, inc=1, device_id=(((z + d) % RING) * RING + y, tp), device_id_type=MESH)

    loads[0].wait()
    loads[13].wait()
    loads[14].wait()
    signal = silu(jnp.concatenate([cond[...], ccond[...], jnp.zeros((6, 256), F32)], axis=0)).astype(BF16)
    mine = dot(signal, mw[...], NT)[0:2]
    part[0] = jnp.concatenate([mine, jnp.zeros((2, 128 - CHUNK), F32)], axis=1)
    loads[1].wait()
    loads[3].wait()
    pl.semaphore_wait(barrier, TP * RING - 1 + RING - 1)

    for n in range(1, TP * RING):
        remote(part.at[0], part.at[n], part_s, part_r, beside[n // TP], across[n % TP]).start()
    lats = [remote(lat.at[tp], lat.at[tp], lat_s, lat_r.at[tp], sp, chip(d)) for d in range(1, 4)]
    lats.append(remote(lat.at[tp], lat.at[tp], lat_s, lat_r.at[tp], sp, partner))
    for c in lats:
        c.start()

    loads[9].wait()
    row = lax.broadcasted_iota(jnp.int32, (BLOCK, 128), 0)
    lane = lax.broadcasted_iota(jnp.int32, (BLOCK, 128), 1)
    token = row + sp * BLOCK
    grid_row = token // GRID_W
    where = jnp.where(lane % 64 < 32, grid_row, token - grid_row * GRID_W).astype(F32)
    angle = where * freq[...]
    cosb[...] = jnp.cos(angle)
    sinb[...] = jnp.where(lane % 32 < 16, -jnp.sin(angle), jnp.sin(angle))

    others = part.at[1 : TP * RING]
    remote(others, others, part_s, part_r, sp, tp).wait_recv()
    for d in range(RING):
        total = part[d * TP]
        for n in range(1, TP):
            total = total + part[d * TP + n]
        modg[z, (y + RING - d) % RING] = total
    zs = [
        remote(modg.at[z], modg.at[z], z_s, z_r, ((z + d) % RING) * RING + y, tp)
        for d in range(1, RING)
    ]
    for c in zs:
        c.start()

    for c in loads[4:9] + loads[10:13]:
        c.wait()
    ones = jnp.ones((BLOCK, 128), BF16)
    for j in range(RING):
        vx[j, :, 128:256] = ones
    vx[RING, :, 128:256] = ones
    for d in range(1, 4):
        slot = chip(d)
        remote(lat.at[slot], lat.at[slot], lat_s, lat_r.at[slot], sp, tp).wait_recv()
        remote(lat.at[slot], lat.at[slot], lat_s, lat_r.at[slot], sp, partner).start()

    wos = [remote(wo.at[tp], wo.at[tp], wo_s, wo_r.at[tp], sp, chip(d)) for d in (1, 3)]
    wos.append(remote(wo.at[tp], wo.at[tp], wo_s, wo_r.at[tp], sp, partner))
    for c in wos:
        c.start()
    for d in range(4):
        slot = ((x + d) % 4) * 2 + 1 - core
        remote(lat.at[slot], lat.at[slot], lat_s, lat_r.at[slot], sp, tp).wait_recv()
    loads[2].wait()

    def norm(v):
        return v * lax.rsqrt(jnp.mean(v * v, axis=1, keepdims=True) + EPSILON)

    nctx[...] = norm(ctx[...].astype(F32))

    def norm_rows(i, carry):
        rows = pl.ds(pl.multiple_of(i * ROWS, ROWS), ROWS)
        nlat[rows, :] = norm(lat[i].astype(F32))
        return carry

    lax.fori_loop(0, TP, norm_rows, 0)
    far_rows = modg.at[0 : RING - 1]
    remote(far_rows, far_rows, z_s, z_r, sp, tp).wait_recv()

    lane2 = lax.broadcasted_iota(jnp.int32, (2, 128), 1)
    for g in range(16):
        c0, c1, c2, c3 = [modg[g // 2, (g % 2) * 4 + j] for j in range(4)]
        c1, c2, c3 = pltpu.roll(c1, 96, 1), pltpu.roll(c2, 64, 1), pltpu.roll(c3, 32, 1)
        rows = [jnp.where(lane2 < 96, c0, c1), jnp.where(lane2 < 64, c1, c2), jnp.where(lane2 < 32, c2, c3)]
        for m in range(3):
            for r in range(2):
                modv[r, 3 * g + m : 3 * g + m + 1, :] = rows[m][r : r + 1]

    qk, val = None, None
    pad = jnp.zeros((CTX, 256), F32)
    for c in range(WIDTH // 256):
        cols = slice(c * 256, (c + 1) * 256)
        pieces = []
        for r, n in ((0, nlat), (1, nctx)):
            scale = jnp.concatenate([modv[r, 16 + 2 * c : 17 + 2 * c, :], modv[r, 17 + 2 * c : 18 + 2 * c, :]], axis=1)
            shift = jnp.concatenate([modv[r, 2 * c : 2 * c + 1, :], modv[r, 2 * c + 1 : 2 * c + 2, :]], axis=1)
            pieces.append(n[:, cols] * (1.0 + scale) + shift)
        h = jnp.concatenate(pieces + [pad], axis=0).astype(BF16)
        one, two = dot(h, wqk[:, cols], NT), dot(h, wval[cols, :])
        qk, val = (one, two) if qk is None else (qk + one, val + two)
    cosine, sine = cosb[...], sinb[...]

    def rope(v):
        turned = jnp.where(lane % 32 < 16, pltpu.roll(v, 112, 1), pltpu.roll(v, 16, 1))
        return v * cosine + turned * sine

    def pass_on(src, dst, send, recv, to):
        remote(src, dst, send, recv, to, tp).start()

    a_up, a_down = at_a((a + 1) % RING), at_a((a + RING - 1) % RING)
    b_up, b_down = at_b((b + 1) % RING), at_b((b + RING - 1) % RING)

    def cut(buf, slot, c):
        if buf.shape[1] == BLOCK:
            return buf.at[slot, c * 128 : (c + 1) * 128]
        return buf.at[slot, 144 * c : 144 + 128 * c]

    def pass_query(near, far, c):
        to = a_up if far + c < 5 else a_down
        pass_on(cut(qb, near, c), cut(qb, far, c), q_s, q_r.at[c, far], to)

    def pass_key(near, far, c):
        pass_on(cut(kb, near, c), cut(kb, far, c), k_s, k_r.at[c, far], b_up if far < 5 else b_down)

    def pass_value(near, far, c):
        pass_on(cut(vb, near, c), cut(vb, far, c), v_s, v_r.at[c, far], b_up if far < 4 else b_down)

    def arrived(buf, recv, slot, c):
        here = cut(buf, slot, c)
        remote(here, here, q_s, recv.at[c, slot], sp, tp).wait_recv()

    qb[0] = (rope(qk[0:BLOCK, 0:128]) * (LOG2E / 8.0)).astype(BF16)
    kb[0, 0:BLOCK, :] = rope(qk[0:BLOCK, 128:256]).astype(BF16)
    kb[0, BLOCK:KEYS, :] = qk[BLOCK:KEYS, 128:256].astype(BF16)
    vb[0] = val.astype(BF16)
    for c in range(2):
        for slot in (1, 7):
            pass_query(0, slot, c)
            pass_key(0, slot, c)
            pass_value(0, slot, c)
    def ring_step(pairs):
        for c in range(2):
            for near, far in pairs:
                arrived(qb, q_r, near, c)
                pass_query(near, far, c)
            for near, far in pairs:
                arrived(kb, k_r, near, c)
                pass_key(near, far, c)
            for near, far in pairs:
                arrived(vb, v_r, near, c)
                pass_value(near, far, c)

    ring_step(((1, 2), (7, 6)))

    lane1 = lax.broadcasted_iota(jnp.int32, (1, 128), 1)
    bias = jnp.where(lane1 % 16 < CTX, boost[0] * LOG2E, -1e30)

    def attend(query, slots, with_context, before):
        scores = [dot(query, kb[j, 0:BLOCK, :], NT) for j in slots]
        peak = scores[0]
        for s in scores[1:]:
            peak = jnp.maximum(peak, s)
        peak = jnp.maximum(peak[:, 0:128], peak[:, 128:256])
        if with_context:
            extra = dot(query, kc[...], NT) + bias
            peak = jnp.maximum(peak, extra)
        if before is not None:
            peak = jnp.maximum(peak, before[1])
        peak = jnp.max(peak, axis=1, keepdims=True)
        acc = None
        if before is not None:
            fade = jnp.exp2(before[1] - peak)
            acc = before[0] * jnp.concatenate([fade, fade], axis=1)
        terms = [(s, vx[j]) for j, s in zip(slots, scores)]
        if with_context:
            terms.append((extra, vx[RING, 0:128, :]))
        for s, v in terms:
            term = dot(jnp.exp2(s - peak).astype(BF16), v)
            acc = term if acc is None else acc + term
        return acc, jnp.broadcast_to(peak, (BLOCK, 128))

    def work(slot, slots, with_context=False, again=False):
        query = qb[slot]
        none = jnp.zeros_like(query)
        for m in range(2):
            masked = jnp.where(lane < 64, query, none) if m == 0 else jnp.where(lane < 64, none, query)
            before = (held[slot, m], top[slot, m]) if again else None
            held[slot, m], top[slot, m] = attend(masked, slots, with_context, before)

    def take_in(slot, box):
        remote(ssend.at[0], srecv.at[box], st_s, st_r.at[box], sp, tp).wait_recv()
        remote(osend.at[0], orecv.at[box], o_s, o_r.at[box], sp, tp).wait_recv()
        theirs = jnp.transpose(jnp.concatenate([srecv[box]] * 16, axis=0))
        for m in range(2):
            mine = top[slot, m]
            their_top = theirs[:, 4 * m : 4 * m + 1]
            new = jnp.maximum(mine, their_top)
            up, down = jnp.exp2(mine - new), jnp.exp2(their_top - new)
            now = held[slot, m]
            held[slot, m, :, 0:128] = now[:, 0:128] * up + orecv[box, :, m * 128 : (m + 1) * 128].astype(F32) * down
            held[slot, m, :, 128:256] = now[:, 128:256] * up + theirs[:, 4 * m + 2 : 4 * m + 3] * down
            top[slot, m] = new

    def stats(slot):
        where = lane % 8
        one = jnp.where(where < 2, top[slot, 0], held[slot, 0, :, 128:256])
        two = jnp.where(where < 6, top[slot, 1], held[slot, 1, :, 128:256])
        return jnp.transpose(jnp.where(where < 4, one, two))[0:8, :]

    def send_off(slot, box, to):
        osend[slot, :, 0:128] = held[slot, 0, :, 0:128].astype(BF16)
        osend[slot, :, 128:256] = held[slot, 1, :, 0:128].astype(BF16)
        ssend[slot] = stats(slot)
        to = at_a((a + to) % RING)
        remote(osend.at[slot], orecv.at[box], o_s, o_r.at[box], to, tp).start()
        remote(ssend.at[slot], srecv.at[box], st_s, st_r.at[box], to, tp).start()

    def unpack(slots):
        for j in slots:
            vx[j, :, 0:128] = vb[j, 0:BLOCK]

    unpack((0, 1, 7))
    work(0, (0, 1, 7))
    work(1, (0, 1, 7))
    ring_step(((2, 3), (6, 5)))

    def share(d):
        remote(wo.at[chip(d)], wo.at[chip(d)], wo_s, wo_r.at[chip(d)], sp, partner).start()

    for c, d in ((0, 3), (1, 1)):
        slot = chip(d)
        remote(wo.at[slot], wo.at[slot], wo_s, wo_r.at[slot], sp, tp).wait_recv()
        piece = wo.at[slot, c * 64 : (c + 1) * 64]
        remote(piece, piece, wo_s, wo2_r.at[c], sp, chip(4 - d)).start()
    share(3)
    unpack((2, 6))
    for slot in (7, 2, 6):
        work(slot, (0, 1, 7, 2, 6))
    for c in range(2):
        arrived(qb, q_r, 3, c)
        arrived(qb, q_r, 5, c)
        pass_query(3 if c == 0 else 5, 4, c)
        arrived(kb, k_r, 3, c)
        pass_key(3, 4, c)
        arrived(vb, v_r, 5, c)
        pass_value(5, 4, c)
        arrived(kb, k_r, 5, c)
        arrived(vb, v_r, 3, c)
    share(1)
    unpack((3, 5))
    for slot in (5, 3):
        work(slot, (0, 1, 7, 2, 6, 3, 5))
    for c in range(2):
        arrived(qb, q_r, 4, c)
        arrived(kb, k_r, 4, c)
        arrived(vb, v_r, 4, c)
    unpack((4,))
    for j in range(RING):
        kc[j * 16 : (j + 1) * 16, :] = kb[j, BLOCK:KEYS]
        vx[RING, j * 16 : (j + 1) * 16, 0:128] = vb[j, BLOCK:KEYS]
    work(4, tuple(range(RING)), True)
    send_off(4, 3, 7)
    work(5, (4,), True, True)
    send_off(5, 5, 1)
    work(2, (3, 5, 4), True, True)
    send_off(2, 2, 6)
    work(3, (4,), True, True)
    take_in(3, 3)
    send_off(3, 4, 5)
    work(6, (3, 5, 4), True, True)
    take_in(6, 5)
    send_off(6, 6, 2)
    for c in range(2):
        piece = wo.at[chip(2), c * 64 : (c + 1) * 64]
        remote(piece, piece, wo_s, wo2_r.at[c], sp, tp).wait_recv()
    share(2)
    work(1, (2, 6, 3, 5, 4), True, True)
    send_off(1, 1, 7)
    work(7, (3, 5, 4), True, True)
    send_off(7, 7, 1)
    work(0, (2, 6, 3, 5, 4), True, True)

    boxes = (7, 2, 1, 6, 4)
    for d in boxes:
        remote(ssend.at[0], srecv.at[d], st_s, st_r.at[d], sp, tp).wait_recv()
    levels = [stats(0)] + [srecv[d] for d in boxes]
    peak = levels[0]
    for v in levels[1:]:
        peak = jnp.maximum(peak, v)
    shares = [jnp.exp2(v - peak) for v in levels]
    sums = None
    for v, share in zip(levels, shares):
        term = share * pltpu.roll(v, 6, 0)
        sums = term if sums is None else sums + term
    first_half = lax.broadcasted_iota(jnp.int32, (8, BLOCK), 0) < 4
    factor = jnp.where(first_half, 1.0, -lam[0]) / sums
    rows = [v * factor for v in shares]
    weights = jnp.transpose(jnp.concatenate(rows + rows[0:1] * 10, axis=0))
    for d in boxes:
        remote(osend.at[0], orecv.at[d], o_s, o_r.at[d], sp, tp).wait_recv()
    mixed = jnp.zeros((BLOCK, 128), F32)
    for n, d in enumerate((0,) + boxes):
        for m in range(2):
            u = held[0, m, :, 0:128] if n == 0 else orecv[d, :, m * 128 : (m + 1) * 128].astype(F32)
            mixed = mixed + u * weights[:, 8 * n + 4 * m : 8 * n + 4 * m + 1]
    normed = mixed * lax.rsqrt(jnp.mean(mixed * mixed, axis=1, keepdims=True) + EPSILON) * gain[...]
    hsend[...] = normed.astype(BF16).reshape(TP, ROWS, 128)
    hs = [
        remote(hsend.at[(tp + d) % TP], hrecv.at[tp], h_s, h_r, sp, (tp + d) % TP)
        for d in range(1, TP)
    ]
    for c in hs:
        c.start()
    hrecv[tp] = hsend[tp]
    for d in range(4):
        slot = ((x + d) % 4) * 2 + 1 - core
        remote(wo.at[slot], wo.at[slot], wo_s, wo_r.at[slot], sp, tp).wait_recv()
    rest = hrecv.at[0 : TP - 1]
    remote(rest, rest, h_s, h_r, sp, tp).wait_recv()
    heads = jnp.concatenate([hrecv[j] for j in range(TP)], axis=1)
    for k in range(WIDTH // 256):
        cols = slice(k * 256, (k + 1) * 256)
        branch = dot(heads, wo[:, :, cols].reshape(TP * 128, 256))
        gate = jnp.concatenate([modv[0, 32 + 2 * k : 33 + 2 * k, :], modv[0, 33 + 2 * k : 34 + 2 * k, :]], axis=1)
        rows_out[:, cols] = (lat[tp, :, cols].astype(F32) + gate * branch).astype(BF16)
        pltpu.make_async_copy(rows_out.at[:, cols], out.at[:, cols], store).start()

    for sent, sem in (
        (others, part_s), (lat.at[1:8], lat_s), (wo.at[1:8], wo_s), (far_rows, z_s), (qb.at[1:8], q_s), (kb.at[1:8], k_s),
        (vb.at[1:8], v_s), (osend.at[1:8], o_s), (ssend.at[1:8], st_s), (rest, h_s),
    ):
        remote(sent, sent, sem, part_r, sp, tp).wait_send()
    pltpu.make_async_copy(rows_out, out, store).wait()


def body(
    latent, context, condition, context_condition, modulation_weight, query_first, query_second, key_first,
    key_second, value_weight, lambda_head, context_score_boost, head_gain, output_weight,
):
    freq = jnp.asarray(np.tile(THETA ** (-np.arange(16, dtype=np.float32) / 16), 8)[None].astype(np.float32))
    hbm = pl.BlockSpec(memory_space=pl.ANY)
    dma = pltpu.SemaphoreType.DMA
    return pl.pallas_call(
        kernel,
        out_shape=jax.ShapeDtypeStruct((ROWS, WIDTH), BF16),
        in_specs=[hbm] * 15,
        out_specs=hbm,
        scratch_shapes=[
            pltpu.VMEM((1, 256), F32),
            pltpu.VMEM((1, 256), F32),
            pltpu.VMEM((1, 128), F32),
            pltpu.VMEM((1, 128), F32),
            pltpu.SMEM((1,), F32),
            pltpu.SMEM((1,), F32),
            pltpu.VMEM((ROWS, WIDTH), BF16),
            pltpu.VMEM((TP, ROWS, WIDTH), BF16),
            pltpu.VMEM((CTX, WIDTH), BF16),
            pltpu.VMEM((CHUNK, 256), BF16),
            pltpu.VMEM((256, WIDTH), BF16),
            pltpu.VMEM((WIDTH, 128), BF16),
            pltpu.VMEM((TP, 128, WIDTH), BF16),
            pltpu.VMEM((TP * RING, 2, 128), F32),
            pltpu.VMEM((RING, RING, 2, 128), F32),
            pltpu.VMEM((2, 48, 128), F32),
            pltpu.VMEM((BLOCK, WIDTH), F32),
            pltpu.VMEM((CTX, WIDTH), F32),
            pltpu.VMEM((BLOCK, 128), F32),
            pltpu.VMEM((BLOCK, 128), F32),
            pltpu.VMEM((RING, BLOCK, 128), BF16),
            pltpu.VMEM((RING, KEYS, 128), BF16),
            pltpu.VMEM((RING, KEYS, 128), BF16),
            pltpu.VMEM((RING + 1, BLOCK, 256), BF16),
            pltpu.VMEM((128, 128), BF16),
            pltpu.VMEM((RING, 2, BLOCK, 256), F32),
            pltpu.VMEM((RING, 2, BLOCK, 128), F32),
            pltpu.VMEM((RING, BLOCK, 256), BF16),
            pltpu.VMEM((RING, 8, BLOCK), F32),
            pltpu.VMEM((RING, BLOCK, 256), BF16),
            pltpu.VMEM((RING, 8, BLOCK), F32),
            pltpu.VMEM((TP, ROWS, 128), BF16),
            pltpu.VMEM((TP, ROWS, 128), BF16),
            dma((15,)), dma(()), dma(()), dma(()), dma(()), dma(()), dma(()), dma((8,)), dma(()), dma((8,)), dma((2,)),
            dma(()), dma((2, 8)), dma(()), dma((2, 8)), dma(()), dma((2, 8)),
            dma(()), dma((8,)), dma(()), dma((8,)), dma(()), dma(()),
        ],
        compiler_params=pltpu.CompilerParams(
            collective_id=0, has_side_effects=True, vmem_limit_bytes=60 * 2**20
        ),
        name="whole",
    )(
        latent, context, condition.reshape(1, 256), context_condition.reshape(1, 256), modulation_weight.T,
        query_first.T, query_second.T, key_first.T, key_second.T, value_weight, lambda_head, context_score_boost,
        head_gain.reshape(1, 128), output_weight, freq,
    )


def solution(mesh):
    in_specs = (
        P(("sp", "tp"), None), P("sp", None), P("tp"), P("tp"), P("tp", "sp"), P(None, "tp"), P(None, "tp"),
        P(None, "tp"), P(None, "tp"), P(None, "tp"), P("tp"), P("tp"), P(), P("tp", None),
    )
    out_specs = P(("sp", "tp"), None)
    return jax.shard_map(body, mesh=mesh, in_specs=in_specs, out_specs=out_specs, check_vma=False)
```

```python
import functools
import math

import jax
import jax.numpy as jnp
import numpy as np
from jax import lax
from jax.experimental import pallas as pl
from jax.experimental.pallas import tpu as pltpu
from jax.sharding import PartitionSpec as P

MESH = pl.DeviceIdType.MESH
EPSILON = 1e-06
THETA = 10000.0
GRID_W = 64
RING = 8
TP = 8
ROWS = 32
BLOCK = 256
CTX = 8
KEYS = BLOCK + 2 * CTX
WIDTH = 2048
CHUNK = 96
LOG2E = math.log2(math.e)
BF16 = jnp.bfloat16
F32 = jnp.float32

NT = (((1,), (1,)), ((), ()))
NN = (((1,), (0,)), ((), ()))


def dot(a, b, dims=NN):
    return lax.dot_general(a, b, dims, preferred_element_type=F32)


def remote(src, dst, send, recv, sp, tp):
    return pltpu.make_async_remote_copy(
        src_ref=src, dst_ref=dst, send_sem=send, recv_sem=recv, device_id=(sp, tp), device_id_type=MESH
    )


def silu(v):
    return v / (1.0 + jnp.exp(-v))


def kernel(
    latent, context, cond_in, ccond_in, modw, wq1, wq2, wk1, wk2, wv, lam_in, boost_in, gain_in, wout, freq_in,
    out,
    cond, ccond, gain, freq, lam, boost,
    lat, ctx, mw, wqk, wval, wo, part, modg, modv, nlat, nctx, cosb, sinb, qb, kb, vb, vx, kc,
    held, top, osend, ssend, orecv, srecv, hsend, hrecv,
    load, part_s, part_r, z_s, z_r, lat_s, lat_r, wo_s, wo_r, wo2_r,
    q_s, q_r, k_s, k_r, v_s, v_r, o_s, o_r, st_s, st_r, h_s, h_r,
):
    sp, tp = lax.axis_index("sp"), lax.axis_index("tp")
    z, y = sp // RING, sp % RING
    x, core = tp // 2, tp % 2
    partner = x * 2 + 1 - core
    a = core * z + (1 - core) * y
    b = core * y + (1 - core) * z

    def at_a(i):
        return (1 - core) * (z * RING + i) + core * (i * RING + y)

    def at_b(i):
        return (1 - core) * (i * RING + y) + core * (z * RING + i)

    def chip(d):
        return ((x + d) % 4) * 2 + core

    loads = [
        pltpu.make_async_copy(modw, mw, load.at[0]),
        pltpu.make_async_copy(latent, lat.at[tp], load.at[1]),
        pltpu.make_async_copy(context, ctx, load.at[2]),
        pltpu.make_async_copy(wout, wo.at[tp], load.at[3]),
        pltpu.make_async_copy(wq1, wqk.at[0:64], load.at[4]),
        pltpu.make_async_copy(wq2, wqk.at[64:128], load.at[5]),
        pltpu.make_async_copy(wk1, wqk.at[128:192], load.at[6]),
        pltpu.make_async_copy(wk2, wqk.at[192:256], load.at[7]),
        pltpu.make_async_copy(wv, wval, load.at[8]),
        pltpu.make_async_copy(freq_in, freq, load.at[9]),
        pltpu.make_async_copy(gain_in, gain, load.at[10]),
        pltpu.make_async_copy(lam_in, lam, load.at[11]),
        pltpu.make_async_copy(boost_in, boost, load.at[12]),
        pltpu.make_async_copy(cond_in, cond, load.at[13]),
        pltpu.make_async_copy(ccond_in, ccond, load.at[14]),
    ]
    for c in loads:
        c.start()

    barrier = pltpu.get_barrier_semaphore()

    beside = [z * RING + (y + d) % RING for d in range(RING)]
    across = [(tp + d) % TP for d in range(TP)]
    for n in range(1, TP * RING):
        pl.semaphore_signal(barrier, inc=1, device_id=(beside[n // TP], across[n % TP]), device_id_type=MESH)
    for d in range(1, RING):
        pl.semaphore_signal(barrier, inc=1, device_id=(((z + d) % RING) * RING + y, tp), device_id_type=MESH)

    loads[0].wait()
    loads[13].wait()
    loads[14].wait()
    signal = silu(jnp.concatenate([cond[...], ccond[...], jnp.zeros((6, 256), F32)], axis=0)).astype(BF16)
    mine = dot(signal, mw[...], NT)[0:2]
    part[0] = jnp.concatenate([mine, jnp.zeros((2, 128 - CHUNK), F32)], axis=1)
    loads[1].wait()
    loads[3].wait()
    pl.semaphore_wait(barrier, TP * RING - 1 + RING - 1)

    for n in range(1, TP * RING):
        remote(part.at[0], part.at[n], part_s, part_r, beside[n // TP], across[n % TP]).start()
    lats = [remote(lat.at[tp], lat.at[tp], lat_s, lat_r.at[tp], sp, chip(d)) for d in range(1, 4)]
    lats.append(remote(lat.at[tp], lat.at[tp], lat_s, lat_r.at[tp], sp, partner))
    for c in lats:
        c.start()

    loads[9].wait()
    row = lax.broadcasted_iota(jnp.int32, (BLOCK, 128), 0)
    lane = lax.broadcasted_iota(jnp.int32, (BLOCK, 128), 1)
    token = row + sp * BLOCK
    grid_row = token // GRID_W
    where = jnp.where(lane % 64 < 32, grid_row, token - grid_row * GRID_W).astype(F32)
    angle = where * freq[...]
    cosb[...] = jnp.cos(angle)
    sinb[...] = jnp.where(lane % 32 < 16, -jnp.sin(angle), jnp.sin(angle))

    others = part.at[1 : TP * RING]
    remote(others, others, part_s, part_r, sp, tp).wait_recv()
    for d in range(RING):
        total = part[d * TP]
        for n in range(1, TP):
            total = total + part[d * TP + n]
        modg[z, (y + RING - d) % RING] = total
    zs = [
        remote(modg.at[z], modg.at[z], z_s, z_r, ((z + d) % RING) * RING + y, tp)
        for d in range(1, RING)
    ]
    for c in zs:
        c.start()

    for c in loads[4:9] + loads[10:13]:
        c.wait()
    ones = jnp.ones((BLOCK, 128), BF16)
    for j in range(RING):
        vx[j, :, 128:256] = ones
    vx[RING, :, 128:256] = ones
    for d in range(1, 4):
        slot = chip(d)
        remote(lat.at[slot], lat.at[slot], lat_s, lat_r.at[slot], sp, tp).wait_recv()
        remote(lat.at[slot], lat.at[slot], lat_s, lat_r.at[slot], sp, partner).start()

    wos = [remote(wo.at[tp], wo.at[tp], wo_s, wo_r.at[tp], sp, chip(d)) for d in (1, 3)]
    wos.append(remote(wo.at[tp], wo.at[tp], wo_s, wo_r.at[tp], sp, partner))
    for c in wos:
        c.start()
    loads[2].wait()

    def norm(v):
        return v * lax.rsqrt(jnp.mean(v * v, axis=1, keepdims=True) + EPSILON)

    def norm_rows(slot):
        nlat[pl.ds(pl.multiple_of(slot * ROWS, ROWS), ROWS), :] = norm(lat[slot].astype(F32))

    def norm_mine(i, carry):
        norm_rows(i * 2 + core)
        return carry

    def norm_partner(i, carry):
        norm_rows(i * 2 + 1 - core)
        return carry

    nctx[...] = norm(ctx[...].astype(F32))
    lax.fori_loop(0, TP // 2, norm_mine, 0)
    for d in range(4):
        slot = ((x + d) % 4) * 2 + 1 - core
        remote(lat.at[slot], lat.at[slot], lat_s, lat_r.at[slot], sp, tp).wait_recv()
    lax.fori_loop(0, TP // 2, norm_partner, 0)
    far_rows = modg.at[0 : RING - 1]
    remote(far_rows, far_rows, z_s, z_r, sp, tp).wait_recv()

    lane2 = lax.broadcasted_iota(jnp.int32, (2, 128), 1)
    for g in range(16):
        c0, c1, c2, c3 = [modg[g // 2, (g % 2) * 4 + j] for j in range(4)]
        c1, c2, c3 = pltpu.roll(c1, 96, 1), pltpu.roll(c2, 64, 1), pltpu.roll(c3, 32, 1)
        rows = [jnp.where(lane2 < 96, c0, c1), jnp.where(lane2 < 64, c1, c2), jnp.where(lane2 < 32, c2, c3)]
        for m in range(3):
            for r in range(2):
                modv[r, 3 * g + m : 3 * g + m + 1, :] = rows[m][r : r + 1]

    qk, val = None, None
    pad = jnp.zeros((CTX, 256), F32)
    for c in range(WIDTH // 256):
        cols = slice(c * 256, (c + 1) * 256)
        pieces = []
        for r, n in ((0, nlat), (1, nctx)):
            scale = jnp.concatenate([modv[r, 16 + 2 * c : 17 + 2 * c, :], modv[r, 17 + 2 * c : 18 + 2 * c, :]], axis=1)
            shift = jnp.concatenate([modv[r, 2 * c : 2 * c + 1, :], modv[r, 2 * c + 1 : 2 * c + 2, :]], axis=1)
            pieces.append(n[:, cols] * (1.0 + scale) + shift)
        h = jnp.concatenate(pieces + [pad], axis=0).astype(BF16)
        one, two = dot(h, wqk[:, cols], NT), dot(h, wval[cols, :])
        qk, val = (one, two) if qk is None else (qk + one, val + two)
    cosine, sine = cosb[...], sinb[...]

    def rope(v):
        turned = jnp.where(lane % 32 < 16, pltpu.roll(v, 112, 1), pltpu.roll(v, 16, 1))
        return v * cosine + turned * sine

    def pass_on(src, dst, send, recv, to):
        remote(src, dst, send, recv, to, tp).start()

    a_up, a_down = at_a((a + 1) % RING), at_a((a + RING - 1) % RING)
    b_up, b_down = at_b((b + 1) % RING), at_b((b + RING - 1) % RING)

    def cut(buf, slot, c):
        if buf.shape[1] == BLOCK:
            return buf.at[slot, c * 128 : (c + 1) * 128]
        return buf.at[slot, 144 * c : 144 + 128 * c]

    def pass_query(near, far, c):
        to = a_up if far + c < 5 else a_down
        pass_on(cut(qb, near, c), cut(qb, far, c), q_s, q_r.at[c, far], to)

    def pass_key(near, far, c):
        pass_on(cut(kb, near, c), cut(kb, far, c), k_s, k_r.at[c, far], b_up if far < 5 else b_down)

    def pass_value(near, far, c):
        pass_on(cut(vb, near, c), cut(vb, far, c), v_s, v_r.at[c, far], b_up if far < 4 else b_down)

    def arrived(buf, recv, slot, c):
        here = cut(buf, slot, c)
        remote(here, here, q_s, recv.at[c, slot], sp, tp).wait_recv()

    qb[0] = (rope(qk[0:BLOCK, 0:128]) * (LOG2E / 8.0)).astype(BF16)
    kb[0, 0:BLOCK, :] = rope(qk[0:BLOCK, 128:256]).astype(BF16)
    kb[0, BLOCK:KEYS, :] = qk[BLOCK:KEYS, 128:256].astype(BF16)
    vb[0] = val.astype(BF16)
    for c in range(2):
        for slot in (1, 7):
            pass_query(0, slot, c)
            pass_key(0, slot, c)
            pass_value(0, slot, c)
    def ring_step(pairs):
        for c in range(2):
            for near, far in pairs:
                arrived(qb, q_r, near, c)
                pass_query(near, far, c)
            for near, far in pairs:
                arrived(kb, k_r, near, c)
                pass_key(near, far, c)
            for near, far in pairs:
                arrived(vb, v_r, near, c)
                pass_value(near, far, c)

    ring_step(((1, 2), (7, 6)))

    lane1 = lax.broadcasted_iota(jnp.int32, (1, 128), 1)
    bias = jnp.where(lane1 % 16 < CTX, boost[0] * LOG2E, -1e30)

    def attend(query, slots, with_context, before):
        scores = [dot(query, kb[j, 0:BLOCK, :], NT) for j in slots]
        peak = scores[0]
        for s in scores[1:]:
            peak = jnp.maximum(peak, s)
        peak = jnp.maximum(peak[:, 0:128], peak[:, 128:256])
        if with_context:
            extra = dot(query, kc[...], NT) + bias
            peak = jnp.maximum(peak, extra)
        if before is not None:
            peak = jnp.maximum(peak, before[1])
        peak = jnp.max(peak, axis=1, keepdims=True)
        acc = None
        if before is not None:
            fade = jnp.exp2(before[1] - peak)
            acc = before[0] * jnp.concatenate([fade, fade], axis=1)
        terms = [(s, vx[j]) for j, s in zip(slots, scores)]
        if with_context:
            terms.append((extra, vx[RING, 0:128, :]))
        for s, v in terms:
            term = dot(jnp.exp2(s - peak).astype(BF16), v)
            acc = term if acc is None else acc + term
        return acc, jnp.broadcast_to(peak, (BLOCK, 128))

    def work(slot, slots, with_context=False, again=False):
        query = qb[slot]
        none = jnp.zeros_like(query)
        for m in range(2):
            masked = jnp.where(lane < 64, query, none) if m == 0 else jnp.where(lane < 64, none, query)
            before = (held[slot, m], top[slot, m]) if again else None
            held[slot, m], top[slot, m] = attend(masked, slots, with_context, before)

    def take_in(slot, box):
        remote(ssend.at[0], srecv.at[box], st_s, st_r.at[box], sp, tp).wait_recv()
        remote(osend.at[0], orecv.at[box], o_s, o_r.at[box], sp, tp).wait_recv()
        theirs = jnp.transpose(jnp.concatenate([srecv[box]] * 16, axis=0))
        for m in range(2):
            mine = top[slot, m]
            their_top = theirs[:, 4 * m : 4 * m + 1]
            new = jnp.maximum(mine, their_top)
            up, down = jnp.exp2(mine - new), jnp.exp2(their_top - new)
            now = held[slot, m]
            held[slot, m, :, 0:128] = now[:, 0:128] * up + orecv[box, :, m * 128 : (m + 1) * 128].astype(F32) * down
            held[slot, m, :, 128:256] = now[:, 128:256] * up + theirs[:, 4 * m + 2 : 4 * m + 3] * down
            top[slot, m] = new

    def stats(slot):
        where = lane % 8
        one = jnp.where(where < 2, top[slot, 0], held[slot, 0, :, 128:256])
        two = jnp.where(where < 6, top[slot, 1], held[slot, 1, :, 128:256])
        return jnp.transpose(jnp.where(where < 4, one, two))[0:8, :]

    def send_off(slot, box, to):
        osend[slot, :, 0:128] = held[slot, 0, :, 0:128].astype(BF16)
        osend[slot, :, 128:256] = held[slot, 1, :, 0:128].astype(BF16)
        ssend[slot] = stats(slot)
        to = at_a((a + to) % RING)
        remote(osend.at[slot], orecv.at[box], o_s, o_r.at[box], to, tp).start()
        remote(ssend.at[slot], srecv.at[box], st_s, st_r.at[box], to, tp).start()

    def unpack(slots):
        for j in slots:
            vx[j, :, 0:128] = vb[j, 0:BLOCK]

    unpack((0, 1, 7))
    work(0, (0, 1, 7))
    work(1, (0, 1, 7))
    ring_step(((2, 3), (6, 5)))

    def share(d):
        remote(wo.at[chip(d)], wo.at[chip(d)], wo_s, wo_r.at[chip(d)], sp, partner).start()

    for c, d in ((0, 3), (1, 1)):
        slot = chip(d)
        remote(wo.at[slot], wo.at[slot], wo_s, wo_r.at[slot], sp, tp).wait_recv()
        piece = wo.at[slot, c * 64 : (c + 1) * 64]
        remote(piece, piece, wo_s, wo2_r.at[c], sp, chip(4 - d)).start()
    share(3)
    unpack((2, 6))
    for slot in (7, 2, 6):
        work(slot, (0, 1, 7, 2, 6))
    for c in range(2):
        arrived(qb, q_r, 3, c)
        arrived(qb, q_r, 5, c)
        pass_query(3 if c == 0 else 5, 4, c)
        arrived(kb, k_r, 3, c)
        pass_key(3, 4, c)
        arrived(vb, v_r, 5, c)
        pass_value(5, 4, c)
        arrived(kb, k_r, 5, c)
        arrived(vb, v_r, 3, c)
    share(1)
    unpack((3, 5))
    for slot in (5, 3):
        work(slot, (0, 1, 7, 2, 6, 3, 5))
    for c in range(2):
        arrived(qb, q_r, 4, c)
        arrived(kb, k_r, 4, c)
        arrived(vb, v_r, 4, c)
    unpack((4,))
    for j in range(RING):
        kc[j * 16 : (j + 1) * 16, :] = kb[j, BLOCK:KEYS]
        vx[RING, j * 16 : (j + 1) * 16, 0:128] = vb[j, BLOCK:KEYS]
    work(4, tuple(range(RING)), True)
    send_off(4, 3, 1)
    work(3, (4,), True, True)
    send_off(3, 4, 5)
    work(2, (3, 5, 4), True, True)
    send_off(2, 2, 6)
    work(5, (4,), True, True)
    take_in(5, 3)
    send_off(5, 5, 1)
    work(1, (2, 6, 3, 5, 4), True, True)
    send_off(1, 1, 7)
    work(7, (3, 5, 4), True, True)
    send_off(7, 7, 1)
    for c in range(2):
        piece = wo.at[chip(2), c * 64 : (c + 1) * 64]
        remote(piece, piece, wo_s, wo2_r.at[c], sp, tp).wait_recv()
    share(2)
    work(6, (3, 5, 4), True, True)
    take_in(6, 5)
    send_off(6, 6, 2)
    work(0, (2, 6, 3, 5, 4), True, True)

    boxes = (2, 4, 1, 7, 6)
    for d in boxes:
        remote(ssend.at[0], srecv.at[d], st_s, st_r.at[d], sp, tp).wait_recv()
    levels = [stats(0)] + [srecv[d] for d in boxes]
    peak = levels[0]
    for v in levels[1:]:
        peak = jnp.maximum(peak, v)
    shares = [jnp.exp2(v - peak) for v in levels]
    sums = None
    for v, share in zip(levels, shares):
        term = share * pltpu.roll(v, 6, 0)
        sums = term if sums is None else sums + term
    first_half = lax.broadcasted_iota(jnp.int32, (8, BLOCK), 0) < 4
    factor = jnp.where(first_half, 1.0, -lam[0]) / sums
    rows = [v * factor for v in shares]
    weights = jnp.transpose(jnp.concatenate(rows + rows[0:1] * 10, axis=0))
    for d in boxes:
        remote(osend.at[0], orecv.at[d], o_s, o_r.at[d], sp, tp).wait_recv()
    mixed = jnp.zeros((BLOCK, 128), F32)
    for n, d in enumerate((0,) + boxes):
        for m in range(2):
            u = held[0, m, :, 0:128] if n == 0 else orecv[d, :, m * 128 : (m + 1) * 128].astype(F32)
            mixed = mixed + u * weights[:, 8 * n + 4 * m : 8 * n + 4 * m + 1]
    normed = mixed * lax.rsqrt(jnp.mean(mixed * mixed, axis=1, keepdims=True) + EPSILON) * gain[...]
    hsend[...] = normed.astype(BF16).reshape(TP, ROWS, 128)
    hs = [
        remote(hsend.at[(tp + d) % TP], hrecv.at[tp], h_s, h_r, sp, (tp + d) % TP)
        for d in range(1, TP)
    ]
    for c in hs:
        c.start()
    hrecv[tp] = hsend[tp]
    for d in range(4):
        slot = ((x + d) % 4) * 2 + 1 - core
        remote(wo.at[slot], wo.at[slot], wo_s, wo_r.at[slot], sp, tp).wait_recv()
    rest = hrecv.at[0 : TP - 1]
    remote(rest, rest, h_s, h_r, sp, tp).wait_recv()
    heads = jnp.concatenate([hrecv[j] for j in range(TP)], axis=1)
    for k in range(WIDTH // 256):
        cols = slice(k * 256, (k + 1) * 256)
        branch = dot(heads, wo[:, :, cols].reshape(TP * 128, 256))
        gate = jnp.concatenate([modv[0, 32 + 2 * k : 33 + 2 * k, :], modv[0, 33 + 2 * k : 34 + 2 * k, :]], axis=1)
        out[:, cols] = (lat[tp, :, cols].astype(F32) + gate * branch).astype(BF16)

    for sent, sem in (
        (others, part_s), (lat.at[1:8], lat_s), (wo.at[1:8], wo_s), (far_rows, z_s), (qb.at[1:8], q_s), (kb.at[1:8], k_s),
        (vb.at[1:8], v_s), (osend.at[1:8], o_s), (ssend.at[1:8], st_s), (rest, h_s),
    ):
        remote(sent, sent, sem, part_r, sp, tp).wait_send()


def body(
    latent, context, condition, context_condition, modulation_weight, query_first, query_second, key_first,
    key_second, value_weight, lambda_head, context_score_boost, head_gain, output_weight,
):
    freq = jnp.asarray(np.tile(THETA ** (-np.arange(16, dtype=np.float32) / 16), 8)[None].astype(np.float32))
    hbm = pl.BlockSpec(memory_space=pl.ANY)
    dma = pltpu.SemaphoreType.DMA
    return pl.pallas_call(
        kernel,
        out_shape=pltpu.VMEM((ROWS, WIDTH), BF16),
        in_specs=[hbm] * 15,
        out_specs=pl.BlockSpec(memory_space=pltpu.VMEM),
        scratch_shapes=[
            pltpu.VMEM((1, 256), F32),
            pltpu.VMEM((1, 256), F32),
            pltpu.VMEM((1, 128), F32),
            pltpu.VMEM((1, 128), F32),
            pltpu.SMEM((1,), F32),
            pltpu.SMEM((1,), F32),
            pltpu.VMEM((TP, ROWS, WIDTH), BF16),
            pltpu.VMEM((CTX, WIDTH), BF16),
            pltpu.VMEM((CHUNK, 256), BF16),
            pltpu.VMEM((256, WIDTH), BF16),
            pltpu.VMEM((WIDTH, 128), BF16),
            pltpu.VMEM((TP, 128, WIDTH), BF16),
            pltpu.VMEM((TP * RING, 2, 128), F32),
            pltpu.VMEM((RING, RING, 2, 128), F32),
            pltpu.VMEM((2, 48, 128), F32),
            pltpu.VMEM((BLOCK, WIDTH), F32),
            pltpu.VMEM((CTX, WIDTH), F32),
            pltpu.VMEM((BLOCK, 128), F32),
            pltpu.VMEM((BLOCK, 128), F32),
            pltpu.VMEM((RING, BLOCK, 128), BF16),
            pltpu.VMEM((RING, KEYS, 128), BF16),
            pltpu.VMEM((RING, KEYS, 128), BF16),
            pltpu.VMEM((RING + 1, BLOCK, 256), BF16),
            pltpu.VMEM((128, 128), BF16),
            pltpu.VMEM((RING, 2, BLOCK, 256), F32),
            pltpu.VMEM((RING, 2, BLOCK, 128), F32),
            pltpu.VMEM((RING, BLOCK, 256), BF16),
            pltpu.VMEM((RING, 8, BLOCK), F32),
            pltpu.VMEM((RING, BLOCK, 256), BF16),
            pltpu.VMEM((RING, 8, BLOCK), F32),
            pltpu.VMEM((TP, ROWS, 128), BF16),
            pltpu.VMEM((TP, ROWS, 128), BF16),
            dma((15,)), dma(()), dma(()), dma(()), dma(()), dma(()), dma((8,)), dma(()), dma((8,)), dma((2,)),
            dma(()), dma((2, 8)), dma(()), dma((2, 8)), dma(()), dma((2, 8)),
            dma(()), dma((8,)), dma(()), dma((8,)), dma(()), dma(()),
        ],
        compiler_params=pltpu.CompilerParams(
            collective_id=0, has_side_effects=True, vmem_limit_bytes=67043328 - 160 * 1024
        ),
        name="whole",
    )(
        latent, context, condition.reshape(1, 256), context_condition.reshape(1, 256), modulation_weight.T,
        query_first.T, query_second.T, key_first.T, key_second.T, value_weight, lambda_head, context_score_boost,
        head_gain.reshape(1, 128), output_weight, freq,
    )


def solution(mesh):
    in_specs = (
        P(("sp", "tp"), None), P("sp", None), P("tp"), P("tp"), P("tp", "sp"), P(None, "tp"), P(None, "tp"),
        P(None, "tp"), P(None, "tp"), P(None, "tp"), P("tp"), P("tp"), P(), P("tp", None),
    )
    out_specs = P(("sp", "tp"), None)
    return jax.shard_map(body, mesh=mesh, in_specs=in_specs, out_specs=out_specs, check_vma=False)
```

```python
import functools
import math

import jax
import jax.numpy as jnp
import numpy as np
from jax import lax
from jax.experimental import pallas as pl
from jax.experimental.pallas import tpu as pltpu
from jax.sharding import PartitionSpec as P

MESH = pl.DeviceIdType.MESH
EPSILON = 1e-06
THETA = 10000.0
GRID_W = 64
RING = 8
TP = 8
ROWS = 32
BLOCK = 256
CTX = 8
KEYS = BLOCK + 2 * CTX
WIDTH = 2048
CHUNK = 96
LOG2E = math.log2(math.e)
BF16 = jnp.bfloat16
F32 = jnp.float32

NT = (((1,), (1,)), ((), ()))
NN = (((1,), (0,)), ((), ()))


def dot(a, b, dims=NN):
    return lax.dot_general(a, b, dims, preferred_element_type=F32)


def remote(src, dst, send, recv, sp, tp):
    return pltpu.make_async_remote_copy(
        src_ref=src, dst_ref=dst, send_sem=send, recv_sem=recv, device_id=(sp, tp), device_id_type=MESH
    )


def silu(v):
    return v / (1.0 + jnp.exp(-v))


def kernel(
    latent, context, cond_in, ccond_in, modw, wq1, wq2, wk1, wk2, wv, lam_in, boost_in, gain_in, wout, freq_in,
    out,
    cond, ccond, gain, freq, lam, boost, branch,
    lat, ctx, mw, wqk, wval, wo, part, modg, modv, nlat, nctx, cosb, sinb, qb, kb, vb, vx, kc,
    held, top, osend, ssend, orecv, srecv, hsend, hrecv,
    load, part_s, part_r, z_s, z_r, lat_s, lat_r, wo_s, wo_r, wo2_r,
    q_s, q_r, k_s, k_r, v_s, v_r, o_s, o_r, st_s, st_r, h_s, h_r,
):
    sp, tp = lax.axis_index("sp"), lax.axis_index("tp")
    z, y = sp // RING, sp % RING
    x, core = tp // 2, tp % 2
    partner = x * 2 + 1 - core
    a = core * z + (1 - core) * y
    b = core * y + (1 - core) * z

    def at_a(i):
        return (1 - core) * (z * RING + i) + core * (i * RING + y)

    def at_b(i):
        return (1 - core) * (i * RING + y) + core * (z * RING + i)

    def chip(d):
        return ((x + d) % 4) * 2 + core

    loads = [
        pltpu.make_async_copy(modw, mw, load.at[0]),
        pltpu.make_async_copy(latent, lat.at[tp], load.at[1]),
        pltpu.make_async_copy(context, ctx, load.at[2]),
        pltpu.make_async_copy(wout, wo.at[tp], load.at[3]),
        pltpu.make_async_copy(wq1, wqk.at[0:64], load.at[4]),
        pltpu.make_async_copy(wq2, wqk.at[64:128], load.at[5]),
        pltpu.make_async_copy(wk1, wqk.at[128:192], load.at[6]),
        pltpu.make_async_copy(wk2, wqk.at[192:256], load.at[7]),
        pltpu.make_async_copy(wv, wval, load.at[8]),
        pltpu.make_async_copy(freq_in, freq, load.at[9]),
        pltpu.make_async_copy(gain_in, gain, load.at[10]),
        pltpu.make_async_copy(lam_in, lam, load.at[11]),
        pltpu.make_async_copy(boost_in, boost, load.at[12]),
        pltpu.make_async_copy(cond_in, cond, load.at[13]),
        pltpu.make_async_copy(ccond_in, ccond, load.at[14]),
    ]
    for c in loads:
        c.start()

    barrier = pltpu.get_barrier_semaphore()

    beside = [z * RING + (y + d) % RING for d in range(RING)]
    across = [(tp + d) % TP for d in range(TP)]
    for n in range(1, TP * RING):
        pl.semaphore_signal(barrier, inc=1, device_id=(beside[n // TP], across[n % TP]), device_id_type=MESH)
    for d in range(1, RING):
        pl.semaphore_signal(barrier, inc=1, device_id=(((z + d) % RING) * RING + y, tp), device_id_type=MESH)

    loads[0].wait()
    loads[13].wait()
    loads[14].wait()
    signal = silu(jnp.concatenate([cond[...], ccond[...], jnp.zeros((6, 256), F32)], axis=0)).astype(BF16)
    mine = dot(signal, mw[...], NT)[0:2]
    part[0] = jnp.concatenate([mine, jnp.zeros((2, 128 - CHUNK), F32)], axis=1)
    loads[1].wait()
    loads[3].wait()
    pl.semaphore_wait(barrier, TP * RING - 1 + RING - 1)

    for n in range(1, TP * RING):
        remote(part.at[0], part.at[n], part_s, part_r, beside[n // TP], across[n % TP]).start()
    lats = [remote(lat.at[tp], lat.at[tp], lat_s, lat_r.at[tp], sp, chip(d)) for d in range(1, 4)]
    lats.append(remote(lat.at[tp], lat.at[tp], lat_s, lat_r.at[tp], sp, partner))
    for c in lats:
        c.start()

    loads[9].wait()
    row = lax.broadcasted_iota(jnp.int32, (BLOCK, 128), 0)
    lane = lax.broadcasted_iota(jnp.int32, (BLOCK, 128), 1)
    token = row + sp * BLOCK
    grid_row = token // GRID_W
    where = jnp.where(lane % 64 < 32, grid_row, token - grid_row * GRID_W).astype(F32)
    angle = where * freq[...]
    cosb[...] = jnp.cos(angle)
    sinb[...] = jnp.where(lane % 32 < 16, -jnp.sin(angle), jnp.sin(angle))

    others = part.at[1 : TP * RING]
    remote(others, others, part_s, part_r, sp, tp).wait_recv()
    for d in range(RING):
        total = part[d * TP]
        for n in range(1, TP):
            total = total + part[d * TP + n]
        modg[z, (y + RING - d) % RING] = total
    zs = [
        remote(modg.at[z], modg.at[z], z_s, z_r, ((z + d) % RING) * RING + y, tp)
        for d in range(1, RING)
    ]
    for c in zs:
        c.start()

    for c in loads[4:9] + loads[10:13]:
        c.wait()
    ones = jnp.ones((BLOCK, 128), BF16)
    for j in range(RING):
        vx[j, :, 128:256] = ones
    vx[RING, :, 128:256] = ones
    for d in range(1, 4):
        slot = chip(d)
        remote(lat.at[slot], lat.at[slot], lat_s, lat_r.at[slot], sp, tp).wait_recv()
        remote(lat.at[slot], lat.at[slot], lat_s, lat_r.at[slot], sp, partner).start()

    wos = [remote(wo.at[tp], wo.at[tp], wo_s, wo_r.at[tp], sp, chip(d)) for d in (1, 3)]
    wos.append(remote(wo.at[tp], wo.at[tp], wo_s, wo_r.at[tp], sp, partner))
    for c in wos:
        c.start()
    loads[2].wait()

    def norm(v):
        return v * lax.rsqrt(jnp.mean(v * v, axis=1, keepdims=True) + EPSILON)

    def norm_rows(slot):
        nlat[pl.ds(pl.multiple_of(slot * ROWS, ROWS), ROWS), :] = norm(lat[slot].astype(F32))

    def norm_mine(i, carry):
        norm_rows(i * 2 + core)
        return carry

    def norm_partner(i, carry):
        norm_rows(i * 2 + 1 - core)
        return carry

    nctx[...] = norm(ctx[...].astype(F32))
    lax.fori_loop(0, TP // 2, norm_mine, 0)
    for d in range(4):
        slot = ((x + d) % 4) * 2 + 1 - core
        remote(lat.at[slot], lat.at[slot], lat_s, lat_r.at[slot], sp, tp).wait_recv()
    lax.fori_loop(0, TP // 2, norm_partner, 0)
    far_rows = modg.at[0 : RING - 1]
    remote(far_rows, far_rows, z_s, z_r, sp, tp).wait_recv()

    lane2 = lax.broadcasted_iota(jnp.int32, (2, 128), 1)
    for g in range(16):
        c0, c1, c2, c3 = [modg[g // 2, (g % 2) * 4 + j] for j in range(4)]
        c1, c2, c3 = pltpu.roll(c1, 96, 1), pltpu.roll(c2, 64, 1), pltpu.roll(c3, 32, 1)
        rows = [jnp.where(lane2 < 96, c0, c1), jnp.where(lane2 < 64, c1, c2), jnp.where(lane2 < 32, c2, c3)]
        for m in range(3):
            for r in range(2):
                modv[r, 3 * g + m : 3 * g + m + 1, :] = rows[m][r : r + 1]

    qk, val = None, None
    pad = jnp.zeros((CTX, 256), F32)
    for c in range(WIDTH // 256):
        cols = slice(c * 256, (c + 1) * 256)
        pieces = []
        for r, n in ((0, nlat), (1, nctx)):
            scale = jnp.concatenate([modv[r, 16 + 2 * c : 17 + 2 * c, :], modv[r, 17 + 2 * c : 18 + 2 * c, :]], axis=1)
            shift = jnp.concatenate([modv[r, 2 * c : 2 * c + 1, :], modv[r, 2 * c + 1 : 2 * c + 2, :]], axis=1)
            pieces.append(n[:, cols] * (1.0 + scale) + shift)
        h = jnp.concatenate(pieces + [pad], axis=0).astype(BF16)
        one, two = dot(h, wqk[:, cols], NT), dot(h, wval[cols, :])
        qk, val = (one, two) if qk is None else (qk + one, val + two)
    cosine, sine = cosb[...], sinb[...]

    def rope(v):
        turned = jnp.where(lane % 32 < 16, pltpu.roll(v, 112, 1), pltpu.roll(v, 16, 1))
        return v * cosine + turned * sine

    def pass_on(src, dst, send, recv, to):
        remote(src, dst, send, recv, to, tp).start()

    a_up, a_down = at_a((a + 1) % RING), at_a((a + RING - 1) % RING)
    b_up, b_down = at_b((b + 1) % RING), at_b((b + RING - 1) % RING)

    def cut(buf, slot, c):
        if buf.shape[1] == BLOCK:
            return buf.at[slot, c * 128 : (c + 1) * 128]
        return buf.at[slot, 144 * c : 144 + 128 * c]

    def pass_query(near, far, c):
        to = a_up if far + c < 5 else a_down
        pass_on(cut(qb, near, c), cut(qb, far, c), q_s, q_r.at[c, far], to)

    def pass_key(near, far, c):
        pass_on(cut(kb, near, c), cut(kb, far, c), k_s, k_r.at[c, far], b_up if far < 5 else b_down)

    def pass_value(near, far, c):
        pass_on(cut(vb, near, c), cut(vb, far, c), v_s, v_r.at[c, far], b_up if far < 4 else b_down)

    def arrived(buf, recv, slot, c):
        here = cut(buf, slot, c)
        remote(here, here, q_s, recv.at[c, slot], sp, tp).wait_recv()

    qb[0] = (rope(qk[0:BLOCK, 0:128]) * (LOG2E / 8.0)).astype(BF16)
    kb[0, 0:BLOCK, :] = rope(qk[0:BLOCK, 128:256]).astype(BF16)
    kb[0, BLOCK:KEYS, :] = qk[BLOCK:KEYS, 128:256].astype(BF16)
    vb[0] = val.astype(BF16)
    for c in range(2):
        for slot in (1, 7):
            pass_query(0, slot, c)
            pass_key(0, slot, c)
            pass_value(0, slot, c)
    def ring_step(pairs):
        for c in range(2):
            for near, far in pairs:
                arrived(qb, q_r, near, c)
                pass_query(near, far, c)
            for near, far in pairs:
                arrived(kb, k_r, near, c)
                pass_key(near, far, c)
            for near, far in pairs:
                arrived(vb, v_r, near, c)
                pass_value(near, far, c)

    ring_step(((1, 2), (7, 6)))

    lane1 = lax.broadcasted_iota(jnp.int32, (1, 128), 1)
    bias = jnp.where(lane1 % 16 < CTX, boost[0] * LOG2E, -1e30)

    def attend(query, slots, with_context, before):
        scores = [dot(query, kb[j, 0:BLOCK, :], NT) for j in slots]
        peak = scores[0]
        for s in scores[1:]:
            peak = jnp.maximum(peak, s)
        peak = jnp.maximum(peak[:, 0:128], peak[:, 128:256])
        if with_context:
            extra = dot(query, kc[...], NT) + bias
            peak = jnp.maximum(peak, extra)
        if before is not None:
            peak = jnp.maximum(peak, before[1])
        peak = jnp.max(peak, axis=1, keepdims=True)
        acc = None
        if before is not None:
            fade = jnp.exp2(before[1] - peak)
            acc = before[0] * jnp.concatenate([fade, fade], axis=1)
        terms = [(s, vx[j]) for j, s in zip(slots, scores)]
        if with_context:
            terms.append((extra, vx[RING, 0:128, :]))
        for s, v in terms:
            term = dot(jnp.exp2(s - peak).astype(BF16), v)
            acc = term if acc is None else acc + term
        return acc, jnp.broadcast_to(peak, (BLOCK, 128))

    def work(slot, slots, with_context=False, again=False):
        query = qb[slot]
        none = jnp.zeros_like(query)
        for m in range(2):
            masked = jnp.where(lane < 64, query, none) if m == 0 else jnp.where(lane < 64, none, query)
            before = (held[slot, m], top[slot, m]) if again else None
            held[slot, m], top[slot, m] = attend(masked, slots, with_context, before)

    def take_in(slot, box):
        remote(ssend.at[0], srecv.at[box], st_s, st_r.at[box], sp, tp).wait_recv()
        remote(osend.at[0], orecv.at[box], o_s, o_r.at[box], sp, tp).wait_recv()
        theirs = jnp.transpose(jnp.concatenate([srecv[box]] * 16, axis=0))
        for m in range(2):
            mine = top[slot, m]
            their_top = theirs[:, 4 * m : 4 * m + 1]
            new = jnp.maximum(mine, their_top)
            up, down = jnp.exp2(mine - new), jnp.exp2(their_top - new)
            now = held[slot, m]
            held[slot, m, :, 0:128] = now[:, 0:128] * up + orecv[box, :, m * 128 : (m + 1) * 128].astype(F32) * down
            held[slot, m, :, 128:256] = now[:, 128:256] * up + theirs[:, 4 * m + 2 : 4 * m + 3] * down
            top[slot, m] = new

    def stats(slot):
        where = lane % 8
        one = jnp.where(where < 2, top[slot, 0], held[slot, 0, :, 128:256])
        two = jnp.where(where < 6, top[slot, 1], held[slot, 1, :, 128:256])
        return jnp.transpose(jnp.where(where < 4, one, two))[0:8, :]

    def send_off(slot, box, to):
        osend[slot, :, 0:128] = held[slot, 0, :, 0:128].astype(BF16)
        osend[slot, :, 128:256] = held[slot, 1, :, 0:128].astype(BF16)
        ssend[slot] = stats(slot)
        to = at_a((a + to) % RING)
        remote(osend.at[slot], orecv.at[box], o_s, o_r.at[box], to, tp).start()
        remote(ssend.at[slot], srecv.at[box], st_s, st_r.at[box], to, tp).start()

    def unpack(slots):
        for j in slots:
            vx[j, :, 0:128] = vb[j, 0:BLOCK]

    unpack((0, 1, 7))
    work(0, (0, 1, 7))
    work(1, (0, 1, 7))
    ring_step(((2, 3), (6, 5)))

    def share(d):
        remote(wo.at[chip(d)], wo.at[chip(d)], wo_s, wo_r.at[chip(d)], sp, partner).start()

    unpack((2, 6))
    for slot in (7, 2, 6):
        work(slot, (0, 1, 7, 2, 6))
    for c in range(2):
        arrived(qb, q_r, 3, c)
        arrived(qb, q_r, 5, c)
        pass_query(3 if c == 0 else 5, 4, c)
        arrived(kb, k_r, 3, c)
        pass_key(3, 4, c)
        arrived(vb, v_r, 5, c)
        pass_value(5, 4, c)
        arrived(kb, k_r, 5, c)
        arrived(vb, v_r, 3, c)
    for c, d in ((0, 3), (1, 1)):
        slot = chip(d)
        remote(wo.at[slot], wo.at[slot], wo_s, wo_r.at[slot], sp, tp).wait_recv()
        piece = wo.at[slot, c * 64 : (c + 1) * 64]
        remote(piece, piece, wo_s, wo2_r.at[c], sp, chip(4 - d)).start()
    share(3)
    share(1)
    unpack((3, 5))
    for slot in (5, 3):
        work(slot, (0, 1, 7, 2, 6, 3, 5))
    for c in range(2):
        arrived(qb, q_r, 4, c)
        arrived(kb, k_r, 4, c)
        arrived(vb, v_r, 4, c)
    unpack((4,))
    for j in range(RING):
        kc[j * 16 : (j + 1) * 16, :] = kb[j, BLOCK:KEYS]
        vx[RING, j * 16 : (j + 1) * 16, 0:128] = vb[j, BLOCK:KEYS]
    work(4, tuple(range(RING)), True)
    send_off(4, 3, 1)
    work(3, (4,), True, True)
    send_off(3, 4, 5)
    work(2, (3, 5, 4), True, True)
    send_off(2, 2, 6)
    work(5, (4,), True, True)
    take_in(5, 3)
    send_off(5, 5, 1)
    work(1, (2, 6, 3, 5, 4), True, True)
    send_off(1, 1, 7)
    work(7, (3, 5, 4), True, True)
    send_off(7, 7, 1)
    for c in range(2):
        piece = wo.at[chip(2), c * 64 : (c + 1) * 64]
        remote(piece, piece, wo_s, wo2_r.at[c], sp, tp).wait_recv()
    share(2)
    work(6, (3, 5, 4), True, True)
    take_in(6, 5)
    send_off(6, 6, 2)
    work(0, (2, 6, 3, 5, 4), True, True)

    boxes = (2, 4, 1, 7, 6)
    for d in boxes:
        remote(ssend.at[0], srecv.at[d], st_s, st_r.at[d], sp, tp).wait_recv()
    levels = [stats(0)] + [srecv[d] for d in boxes]
    peak = levels[0]
    for v in levels[1:]:
        peak = jnp.maximum(peak, v)
    shares = [jnp.exp2(v - peak) for v in levels]
    sums = None
    for v, share in zip(levels, shares):
        term = share * pltpu.roll(v, 6, 0)
        sums = term if sums is None else sums + term
    first_half = lax.broadcasted_iota(jnp.int32, (8, BLOCK), 0) < 4
    factor = jnp.where(first_half, 1.0, -lam[0]) / sums
    rows = [v * factor for v in shares]
    weights = jnp.transpose(jnp.concatenate(rows + rows[0:1] * 10, axis=0))
    for d in boxes:
        remote(osend.at[0], orecv.at[d], o_s, o_r.at[d], sp, tp).wait_recv()
    mixed = jnp.zeros((BLOCK, 128), F32)
    for n, d in enumerate((0,) + boxes):
        for m in range(2):
            u = held[0, m, :, 0:128] if n == 0 else orecv[d, :, m * 128 : (m + 1) * 128].astype(F32)
            mixed = mixed + u * weights[:, 8 * n + 4 * m : 8 * n + 4 * m + 1]
    normed = mixed * lax.rsqrt(jnp.mean(mixed * mixed, axis=1, keepdims=True) + EPSILON) * gain[...]
    hsend[...] = normed.astype(BF16).reshape(TP, ROWS, 128)
    hs = []
    for d in (2, 1, 3, 0):
        for n in (core, 1 - core) if d else (1 - core,):
            to = ((x + d) % 4) * 2 + n
            hs.append(remote(hsend.at[to], hrecv.at[tp], h_s, h_r.at[1 if d == 2 else 0], sp, to))
    for c in hs:
        c.start()
    hrecv[tp] = hsend[tp]
    for d in range(4):
        slot = ((x + d) % 4) * 2 + 1 - core
        remote(wo.at[slot], wo.at[slot], wo_s, wo_r.at[slot], sp, tp).wait_recv()
    near_heads, far_heads, rest = hrecv.at[0:5], hrecv.at[0:2], hrecv.at[0 : TP - 1]
    remote(near_heads, near_heads, h_s, h_r.at[0], sp, tp).wait_recv()

    def branch_of(d, cols):
        pair = ((x + d) % 4) * 2
        heads = jnp.concatenate([hrecv[pair], hrecv[pair + 1]], axis=1)
        return dot(heads, wo[pl.ds(pair, 2), :, cols].reshape(256, 256))

    for k in range(WIDTH // 256):
        cols = slice(k * 256, (k + 1) * 256)
        branch[:, cols] = branch_of(0, cols) + branch_of(1, cols) + branch_of(3, cols)
    remote(far_heads, far_heads, h_s, h_r.at[1], sp, tp).wait_recv()
    for k in range(WIDTH // 256):
        cols = slice(k * 256, (k + 1) * 256)
        gate = jnp.concatenate([modv[0, 32 + 2 * k : 33 + 2 * k, :], modv[0, 33 + 2 * k : 34 + 2 * k, :]], axis=1)
        out[:, cols] = (lat[tp, :, cols].astype(F32) + gate * (branch[:, cols] + branch_of(2, cols))).astype(BF16)

    for sent, sem in (
        (others, part_s), (lat.at[1:8], lat_s), (wo.at[1:8], wo_s), (far_rows, z_s), (qb.at[1:8], q_s), (kb.at[1:8], k_s),
        (vb.at[1:8], v_s), (osend.at[1:8], o_s), (ssend.at[1:8], st_s), (rest, h_s),
    ):
        remote(sent, sent, sem, part_r, sp, tp).wait_send()


def body(
    latent, context, condition, context_condition, modulation_weight, query_first, query_second, key_first,
    key_second, value_weight, lambda_head, context_score_boost, head_gain, output_weight,
):
    freq = jnp.asarray(np.tile(THETA ** (-np.arange(16, dtype=np.float32) / 16), 8)[None].astype(np.float32))
    hbm = pl.BlockSpec(memory_space=pl.ANY)
    dma = pltpu.SemaphoreType.DMA
    return pl.pallas_call(
        kernel,
        out_shape=pltpu.VMEM((ROWS, WIDTH), BF16),
        in_specs=[hbm] * 15,
        out_specs=pl.BlockSpec(memory_space=pltpu.VMEM),
        scratch_shapes=[
            pltpu.VMEM((1, 256), F32),
            pltpu.VMEM((1, 256), F32),
            pltpu.VMEM((1, 128), F32),
            pltpu.VMEM((1, 128), F32),
            pltpu.SMEM((1,), F32),
            pltpu.SMEM((1,), F32),
            pltpu.VMEM((ROWS, WIDTH), F32),
            pltpu.VMEM((TP, ROWS, WIDTH), BF16),
            pltpu.VMEM((CTX, WIDTH), BF16),
            pltpu.VMEM((CHUNK, 256), BF16),
            pltpu.VMEM((256, WIDTH), BF16),
            pltpu.VMEM((WIDTH, 128), BF16),
            pltpu.VMEM((TP, 128, WIDTH), BF16),
            pltpu.VMEM((TP * RING, 2, 128), F32),
            pltpu.VMEM((RING, RING, 2, 128), F32),
            pltpu.VMEM((2, 48, 128), F32),
            pltpu.VMEM((BLOCK, WIDTH), F32),
            pltpu.VMEM((CTX, WIDTH), F32),
            pltpu.VMEM((BLOCK, 128), F32),
            pltpu.VMEM((BLOCK, 128), F32),
            pltpu.VMEM((RING, BLOCK, 128), BF16),
            pltpu.VMEM((RING, KEYS, 128), BF16),
            pltpu.VMEM((RING, KEYS, 128), BF16),
            pltpu.VMEM((RING + 1, BLOCK, 256), BF16),
            pltpu.VMEM((128, 128), BF16),
            pltpu.VMEM((RING, 2, BLOCK, 256), F32),
            pltpu.VMEM((RING, 2, BLOCK, 128), F32),
            pltpu.VMEM((RING, BLOCK, 256), BF16),
            pltpu.VMEM((RING, 8, BLOCK), F32),
            pltpu.VMEM((RING, BLOCK, 256), BF16),
            pltpu.VMEM((RING, 8, BLOCK), F32),
            pltpu.VMEM((TP, ROWS, 128), BF16),
            pltpu.VMEM((TP, ROWS, 128), BF16),
            dma((15,)), dma(()), dma(()), dma(()), dma(()), dma(()), dma((8,)), dma(()), dma((8,)), dma((2,)),
            dma(()), dma((2, 8)), dma(()), dma((2, 8)), dma(()), dma((2, 8)),
            dma(()), dma((8,)), dma(()), dma((8,)), dma(()), dma((2,)),
        ],
        compiler_params=pltpu.CompilerParams(
            collective_id=0, has_side_effects=True, vmem_limit_bytes=67043328 - 160 * 1024
        ),
        name="whole",
    )(
        latent, context, condition.reshape(1, 256), context_condition.reshape(1, 256), modulation_weight.T,
        query_first.T, query_second.T, key_first.T, key_second.T, value_weight, lambda_head, context_score_boost,
        head_gain.reshape(1, 128), output_weight, freq,
    )


def solution(mesh):
    in_specs = (
        P(("sp", "tp"), None), P("sp", None), P("tp"), P("tp"), P("tp", "sp"), P(None, "tp"), P(None, "tp"),
        P(None, "tp"), P(None, "tp"), P(None, "tp"), P("tp"), P("tp"), P(), P("tp", None),
    )
    out_specs = P(("sp", "tp"), None)
    return jax.shard_map(body, mesh=mesh, in_specs=in_specs, out_specs=out_specs, check_vma=False)
```
